128 devices in a mesh: sp: 32 (over z, y, core), tp: 4 (over x).
Axes of the slice: x: 4, y: 4, z: 4, core: 2. Of those that a mesh axis runs over, the one named last changes fastest.
Arguments:
- tokens: bfloat16 [16384, 2048], P(('sp', 'tp')), may hold values from -6 to 6
- norm_gain: float32 [2048], replicated, may hold values from 0.1 to 1.9
- query_weight: bfloat16 [2048, 1024], P(None, 'tp'), may hold values from -0.13258252 to 0.13258252
- key_weight: bfloat16 [2048, 1024], P(None, 'tp'), may hold values from -0.13258252 to 0.13258252
- value_weight: bfloat16 [2048, 1024], P(None, 'tp'), may hold values from -0.125 to 0.125
- glu_value_weight: bfloat16 [2048, 1024], P(None, 'tp'), may hold values from -0.125 to 0.125
- glu_gate_weight: bfloat16 [2048, 1024], P(None, 'tp'), may hold values from -0.125 to 0.125
- qk_gain: float32 [2, 64], replicated, may hold values from 1 to 6
- mix_lambda: float32 [8], P('tp'), may hold values from 0.3 to 0.8
- head_gain: float32 [128], replicated, may hold values from 0.1 to 1.9
- conv_kernel: float32 [31, 1024], P(None, 'tp'), may hold values from -1 to 1
- channel_gain: float32 [1024], P('tp'), may hold values from 0.1 to 1.9
- channel_shift: float32 [1024], P('tp'), may hold values from -3 to 3
- output_weight: bfloat16 [2048, 2048], replicated, may hold values from -0.125 to 0.125
Outputs:
- mixed: bfloat16 [16384, 2048], P(('sp', 'tp'))
- log_totals: float32 [2, 8, 16384], P(None, 'tp', 'sp')
The draws below stay inside these ranges and needn't reach their ends.
All inputs are finite; a program needn't handle non-finite values.
Results may differ from the reference program's by a relative error of at most 0.035.
Values may be sent and summed in bfloat16 or wider, within the bound.
No kernel may reach another device: no remote copies, remote signals or barrier semaphores. Data moves between devices by JAX's collectives and lax.ppermute only.
A program may use at most 128 MiB of HBM per device.

```python
import jax
import jax.numpy as jnp
from jax import lax

D = 2048
HEADS = 8
HEAD_DIM = 64
VDIM = 128
CONV = 1024
KERNEL = 31
TOKENS = 16384
MIX = 2048


def draw_qk_gain(key, part):
    spread = jax.random.uniform(jax.random.fold_in(key, 7), (2, HEAD_DIM), jnp.float32, -1.0, 1.0)
    return 1.3 + 0.25 * spread


def paired_weights(key):
    columns = HEADS * 2 * HEAD_DIM
    factor = D ** (-0.5)
    limit = 6.0 * factor
    shared = jax.random.normal(jax.random.fold_in(key, 11), (D, columns), jnp.float32) * factor
    separate = jax.random.normal(jax.random.fold_in(key, 12), (D, columns), jnp.float32) * factor
    shared = jnp.clip(shared, -limit, limit)
    separate = jnp.clip(separate, -limit, limit)
    return (shared, separate)


def draw_query_weight(key, part):
    shared, separate = paired_weights(key)
    return shared.astype(jnp.bfloat16)


def draw_key_weight(key, part):
    shared, separate = paired_weights(key)
    return separate.astype(jnp.bfloat16)


def block_levels(rng, dims, pieces, low, largest):
    def one(position, blocks):
        draws = jax.random.uniform(jax.random.fold_in(jax.random.fold_in(rng, 6), position), (blocks,), jnp.float32, low / len(pieces), largest / len(pieces))
        return jnp.repeat(jnp.exp(draws), dims[position] // blocks).reshape((-1,) + (1,) * (len(dims) - position - 1))

    factor_of = one(*pieces[0])
    for cut in pieces[1:]:
        factor_of = factor_of * one(*cut)
    return factor_of


def normal_values(own_key, shape, width, most, split=(), held_as=jnp.bfloat16):
    drawn = width * jax.random.normal(own_key, shape, jnp.float32)
    if split:
        drawn = drawn * block_levels(own_key, shape, split, -0.22, 0.18)
    return jnp.clip(drawn, -most, most).astype(held_as)


def setup_inputs(seed: int = 0) -> dict:
    splits = jax.random.split(jax.random.key(seed), 15)
    tokens = normal_values(splits[0], (TOKENS, D), 1.0, 6.0, ((0, 128),))
    norm_gain = jnp.clip(1.0 + 0.18 * jax.random.normal(splits[1], (D,), jnp.float32), 0.1, 1.9)
    query_weight = draw_query_weight(jax.random.fold_in(splits[14], 71), 0)
    key_weight = draw_key_weight(jax.random.fold_in(splits[14], 71), 0)
    value_weight = normal_values(splits[4], (D, HEADS * VDIM), D ** -0.5, 0.125, ((1, 4),))
    glu_value_weight = normal_values(splits[5], (D, CONV), D ** -0.5, 0.125, ((1, 4),))
    glu_gate_weight = normal_values(splits[6], (D, CONV), D ** -0.5, 0.125, ((1, 4),))
    qk_gain = draw_qk_gain(jax.random.fold_in(splits[14], 71), 0)
    mix_lambda = jnp.clip(0.3 + 0.5 * jax.random.uniform(splits[8], (HEADS,), jnp.float32) ** block_levels(splits[8], (HEADS,), ((0, 4),), -0.2, 0.2), 0.3, 0.8)
    head_gain = jnp.clip(1.0 + 0.18 * jax.random.normal(splits[9], (VDIM,), jnp.float32), 0.1, 1.9)
    conv_kernel = normal_values(splits[10], (KERNEL, CONV), KERNEL ** -0.5, 1.0, ((1, 4),), jnp.float32)
    channel_gain = jnp.clip(1.0 + 0.18 * jax.random.normal(splits[11], (CONV,), jnp.float32), 0.1, 1.9)
    channel_shift = normal_values(splits[12], (CONV,), 0.5, 3.0, ((0, 4),), jnp.float32)
    output_weight = normal_values(splits[13], (MIX, D), MIX ** -0.5, 0.125)
    return dict(tokens=tokens, norm_gain=norm_gain, query_weight=query_weight, key_weight=key_weight, value_weight=value_weight, glu_value_weight=glu_value_weight, glu_gate_weight=glu_gate_weight, qk_gain=qk_gain, mix_lambda=mix_lambda, head_gain=head_gain, conv_kernel=conv_kernel, channel_gain=channel_gain, channel_shift=channel_shift, output_weight=output_weight)


def rotate(values, positions):
    half = values.shape[-1] // 2
    inverse = 10000.0 ** (-jnp.arange(0, half, dtype=jnp.float32) * 2.0 / values.shape[-1])
    angles = positions[:, None] * inverse[None, :]
    cosine = jnp.cos(angles)[:, None, None, :]
    sine = jnp.sin(angles)[:, None, None, :]
    first = values[..., :half]
    second = values[..., half:]
    return jnp.concatenate([first * cosine - second * sine, second * cosine + first * sine], axis=-1)

def prepare(raw, qk_gain, positions):
    values = raw.astype(jnp.float32)
    values = values * lax.rsqrt(lax.optimization_barrier(jnp.mean(values * values, axis=-1, keepdims=True)) + 1e-06)
    values = values * qk_gain[None, None, :, :]
    return rotate(values, positions).astype(jnp.bfloat16)

def reference(tokens, norm_gain, query_weight, key_weight, value_weight, glu_value_weight, glu_gate_weight, qk_gain, mix_lambda, head_gain, conv_kernel, channel_gain, channel_shift, output_weight):
    inputs = tokens.astype(jnp.float32)
    normed = (inputs * lax.rsqrt(lax.optimization_barrier(jnp.mean(inputs * inputs, axis=-1, keepdims=True)) + 1e-06) * norm_gain).astype(jnp.bfloat16)
    queries = jnp.dot(normed, query_weight, preferred_element_type=jnp.float32).astype(jnp.bfloat16).reshape(TOKENS, HEADS, 2, HEAD_DIM)
    keys = jnp.dot(normed, key_weight, preferred_element_type=jnp.float32).astype(jnp.bfloat16).reshape(TOKENS, HEADS, 2, HEAD_DIM)
    values = jnp.dot(normed, value_weight, preferred_element_type=jnp.float32).astype(jnp.bfloat16).reshape(TOKENS, HEADS, VDIM)
    glu_a = jnp.dot(normed, glu_value_weight, preferred_element_type=jnp.float32).astype(jnp.bfloat16)
    glu_g = jnp.dot(normed, glu_gate_weight, preferred_element_type=jnp.float32).astype(jnp.bfloat16)
    positions = jnp.arange(TOKENS, dtype=jnp.int32)
    rq = prepare(queries, qk_gain, positions.astype(jnp.float32))
    rk = prepare(keys, qk_gain, positions.astype(jnp.float32))
    key_heads = jnp.transpose(rk, (1, 0, 2, 3)).astype(jnp.float32)
    value_heads = jnp.transpose(values, (1, 0, 2)).astype(jnp.float32)
    block = 512
    blocks = TOKENS // block
    query_blocks = rq.reshape(blocks, block, HEADS, 2, HEAD_DIM)
    starts = jnp.arange(blocks, dtype=jnp.int32) * block
    scale = HEAD_DIM ** (-0.5)

    def one_block(item):
        query_block, begin = item
        query_pos = begin + jnp.arange(block, dtype=jnp.int32)
        allowed = positions[None, :] <= query_pos[:, None]

        def one_head(head_item):
            query_head, key_head, value_head, weight_two = head_item
            scores = jnp.einsum('qmd,kmd->mqk', query_head.astype(jnp.float32), key_head) * scale
            scores = jnp.where(allowed[None], scores, -1e+30)
            top = lax.optimization_barrier(jnp.max(scores, axis=-1))
            probs = jnp.where(allowed[None], jnp.exp(scores - top[..., None]), 0.0)
            total = lax.optimization_barrier(jnp.sum(probs, axis=-1))
            rounded = probs.astype(jnp.bfloat16).astype(jnp.float32)
            summed = jnp.einsum('mqk,kd->mqd', rounded, value_head)
            heads_out = summed[0] / total[0][:, None] - weight_two * summed[1] / total[1][:, None]
            heads_out = heads_out * lax.rsqrt(lax.optimization_barrier(jnp.mean(heads_out * heads_out, axis=-1, keepdims=True)) + 1e-06) * head_gain
            return (heads_out.astype(jnp.bfloat16), top + jnp.log(total))
        return lax.map(one_head, (jnp.transpose(query_block, (1, 0, 2, 3)), key_heads, value_heads, mix_lambda))
    outputs, totals = lax.map(one_block, (query_blocks, starts))
    attended = jnp.transpose(outputs, (0, 2, 1, 3)).reshape(TOKENS, HEADS * VDIM)
    log_totals = jnp.transpose(totals, (2, 1, 0, 3)).reshape(2, HEADS, TOKENS)
    gated = (glu_a.astype(jnp.float32) * jax.nn.sigmoid(glu_g.astype(jnp.float32))).astype(jnp.bfloat16)
    padded = jnp.concatenate([jnp.zeros((KERNEL - 1, CONV), jnp.float32), gated.astype(jnp.float32)], axis=0)
    convolved = jnp.zeros((TOKENS, CONV), jnp.float32)
    for offset in range(KERNEL):
        convolved = convolved + conv_kernel[offset][None, :] * padded[offset:offset + TOKENS]
    middle = lax.optimization_barrier(jnp.mean(convolved, axis=-1, keepdims=True))
    spread = lax.optimization_barrier(jnp.mean(convolved * convolved, axis=-1, keepdims=True)) - middle * middle
    conv_out = jax.nn.silu((convolved - middle) * lax.rsqrt(spread + 1e-05) * channel_gain + channel_shift).astype(jnp.bfloat16)
    merged = jnp.concatenate([attended, conv_out], axis=1)
    mixed = jnp.dot(merged, output_weight, preferred_element_type=jnp.float32).astype(jnp.bfloat16)
    return (mixed, log_totals)
```

```python
import math

import jax
import jax.numpy as jnp
from jax import lax
from jax.experimental import pallas as pl
from jax.experimental.pallas import tpu as pltpu
from jax.sharding import PartitionSpec as P

NZ, NY, NC = 4, 4, 2
BIG = 2.0**100
LOG2E = math.log2(math.e)
BF = jnp.bfloat16
F32 = jnp.float32


def vmem():
    return pl.BlockSpec(memory_space=pltpu.VMEM)


def smem():
    return pl.BlockSpec(memory_space=pltpu.SMEM)


def moves(target):
    out = []
    for z in range(NZ):
        for y in range(NY):
            for c in range(NC):
                t = target(z, y, c)
                if t is not None:
                    out.append(((z * NY + y) * NC + c, (t[0] * NY + t[1]) * NC + t[2]))
    return out


def along_y(value, step):
    return lax.ppermute(value, "sp", moves(lambda z, y, c: (z, (y + step) % NY, c)))


def up_z(value, step):
    return lax.ppermute(
        value, "sp", moves(lambda z, y, c: (z + step, y, c) if z + step < NZ else None)
    )


def to_sibling(value):
    return lax.ppermute(value, "sp", moves(lambda z, y, c: (z, y, 1 - c)))


def along_x(value, step):
    count = lax.axis_size("tp")
    return lax.ppermute(value, "tp", [(i, (i + step) % count) for i in range(count)])


def project_kernel(
    pos, t0, t1, t2, t3, gain, wq, wk, wv, wa, wg, qkg, cos, sin, mine, other, gated, normed
):
    x = pos[3]
    c = pos[2]
    for ref, step in ((t0, 0), (t1, 3), (t2, 1), (t3, 2)):
        t = ref[...].astype(F32)
        ms = jnp.mean(t * t, axis=-1, keepdims=True)
        n = (t * lax.rsqrt(ms + 1e-06) * gain[...]).astype(BF)
        at = pl.multiple_of(lax.rem(x + step, 4) * 128, 128)
        normed[pl.ds(at, 128), :] = n
    lane = lax.broadcasted_iota(jnp.int32, (1, 256), 1)
    first = lax.rem(lane, 64) < 32
    gi = lax.broadcasted_iota(jnp.int32, (256, 256), 0) // 64
    gj = lax.broadcasted_iota(jnp.int32, (256, 256), 1) // 64
    groups = jnp.where(gi == gj, 1.0 / 64, 0.0).astype(BF)

    def times(w):
        return jnp.dot(normed[...], w[...], preferred_element_type=F32).astype(BF).astype(F32)

    def turned(w):
        v = times(w)
        sq = v * v
        hi = sq.astype(BF)
        lo = (sq - hi.astype(F32)).astype(BF)
        ms = jnp.dot(hi, groups, preferred_element_type=F32) + jnp.dot(
            lo, groups, preferred_element_type=F32
        )
        v = v * lax.rsqrt(ms + 1e-06) * qkg[...]
        swapped = jnp.where(first, pltpu.roll(v, 256 - 32, 1), pltpu.roll(v, 32, 1))
        cc = jnp.concatenate([cos[...], cos[...]], axis=1)
        ss = jnp.concatenate([sin[...], sin[...]], axis=1)
        return v * cc + swapped * ss

    def put(row, v, flip, blocks):
        a = v[:, :128]
        b = v[:, 128:]
        for ref, val in ((mine, jnp.where(c == 0, a, b)), (other, jnp.where(c == 0, b, a))):
            if flip:
                ref[row : row + 128, :] = val.T.astype(BF)
            else:
                for i in range(4):
                    ref[row : row + 128, i * 128 : (i + 1) * 128] = val[
                        i * 128 : (i + 1) * 128, :
                    ].astype(BF)

    put(0, turned(wq) * (LOG2E / 8.0), True, 4)
    put(128, turned(wk), False, 4)
    put(256, times(wv), True, 4)
    ga = times(wa)
    gg = times(wg)
    gated[...] = (ga * jax.nn.sigmoid(gg)).astype(BF)


def project(pos, pieces, gain, weights, qkg, cos, sin):
    return pl.pallas_call(
        project_kernel,
        out_shape=(
            jax.ShapeDtypeStruct((384, 512), BF),
            jax.ShapeDtypeStruct((384, 512), BF),
            jax.ShapeDtypeStruct((512, 256), BF),
        ),
        in_specs=[smem()] + [vmem()] * 13,
        out_specs=(vmem(),) * 3,
        scratch_shapes=[pltpu.VMEM((512, 2048), BF)],
        compiler_params=pltpu.CompilerParams(vmem_limit_bytes=40 * 1024 * 1024),
        cost_estimate=pl.CostEstimate(flops=2700000000, bytes_accessed=8000000, transcendentals=0),
        name="project",
    )(pos, *pieces, gain, *weights, qkg, cos, sin)


def conv_kernel_body(gated, halo, taps, out, ext):
    ext[0:32, :] = jnp.zeros((32, 256), F32)
    ext[544:560, :] = jnp.zeros((16, 256), F32)
    ext[2:32, :] = halo[...].astype(F32)
    ext[32:544, :] = gated[...].astype(F32)
    acc = jnp.zeros((512, 256), F32)
    for r in range(8):
        moved = ext[r : r + 544, :]
        for a in range(5):
            j = a * 8 + r - 2
            if 0 <= j < 31:
                acc = acc + taps[j : j + 1, :] * moved[8 * a : 8 * a + 512]
    out[...] = acc.astype(BF)


def convolve(gated, halo, taps):
    return pl.pallas_call(
        conv_kernel_body,
        out_shape=jax.ShapeDtypeStruct((512, 256), BF),
        in_specs=[vmem()] * 3,
        out_specs=vmem(),
        scratch_shapes=[pltpu.VMEM((560, 256), F32)],
        cost_estimate=pl.CostEstimate(flops=4000000000, bytes_accessed=800000, transcendentals=0),
        name="convolve",
    )(gated, halo, taps)


def split3(v):
    hi = v.astype(BF).astype(F32)
    mid = (v - hi).astype(BF).astype(F32)
    return [hi, mid, v - hi - mid]


def attend_kernel(
    pos, q0, q1, q2, q3, kv0, kv1, kv2, kv3, s1, s2, s3, own, stats,
    qz, kscr, vscr, sbuf, pbuf, oacc, tacc, mref, flag,
):
    z = pos[0]
    y = pos[1]
    ysrc = [y, lax.rem(y + 3, 4), lax.rem(y + 1, 4), lax.rem(y + 2, 4)]
    rows = lax.broadcasted_iota(jnp.int32, (128, 1024), 0)
    for s, ref in enumerate((q0, q1, q2, q3)):
        q = ref[...]
        qz[ysrc[s] * 2] = jnp.where(rows < 64, q, jnp.zeros_like(q))
        qz[ysrc[s] * 2 + 1] = jnp.where(rows >= 64, q, jnp.zeros_like(q))
    for b, ref in enumerate((kv0, kv1, kv2, kv3)):
        for i in range(8):
            kscr[b, i * 128 : (i + 1) * 128, :] = ref[0:128, i * 128 : (i + 1) * 128]
        vscr[b] = ref[128:256, :]
    mref[...] = jnp.zeros_like(mref)
    flag[0] = 1
    items = [(m, qt) for m in range(2) for qt in range(4)]
    full = (3 - y) + 4 * z

    def which(t):
        u = t - (3 - y)
        near = u < 0
        return jnp.where(near, 0, 1 + u // 4), jnp.where(near, y + 1 + t, lax.rem(u, 4))

    def score(b, s, m, qt):
        return jnp.dot(
            kscr[b], qz[s * 2 + m, :, qt * 256 : (qt + 1) * 256], preferred_element_type=F32
        )

    def weigh(r, cols, scores, masked):
        n = scores.shape[0]
        p = jnp.exp2(scores.reshape(n // 8, 8, 256) - mref[r, :, cols][None]).reshape(n, 256)
        if masked:
            k = lax.broadcasted_iota(jnp.int32, (256, 256), 0)
            q = lax.broadcasted_iota(jnp.int32, (256, 256), 1)
            last = jnp.where(k <= q, p[n - 256 :], 0.0)
            p = last if n == 256 else jnp.concatenate([p[: n - 256], last], axis=0)
        tacc[r, :, cols] += jnp.sum(p.reshape(n // 8, 8, 256), axis=0)
        return p.astype(BF)

    def pair(t):
        b, s = which(t)
        bn, sn = which(jnp.minimum(t + 1, full - 1))
        for i, (m, qt) in enumerate(items):
            if i + 1 < len(items):
                sbuf[(i + 1) % 2] = score(b, s, *items[i + 1])
            else:
                sbuf[0] = score(bn, sn, 0, 0)
            cols = slice(qt * 256, (qt + 1) * 256)
            r = s * 2 + m
            pbuf[i % 2] = weigh(r, cols, sbuf[i % 2], False)
            oacc[r, :, cols] += jnp.dot(vscr[b], pbuf[i % 2], preferred_element_type=F32)

    def diagonal():
        for i, (m, qt) in enumerate(items):
            n = (qt + 1) * 256
            cols = slice(qt * 256, n)
            r = y * 2 + m
            sbuf[i % 2, :n, :] = jnp.dot(kscr[0, :n, :], qz[r, :, cols], preferred_element_type=F32)
            pbuf[i % 2, :n, :] = weigh(r, cols, sbuf[i % 2, :n, :], True)
            oacc[r, :, cols] += jnp.dot(
                vscr[0, :, :n], pbuf[i % 2, :n, :], preferred_element_type=F32
            )

    def tops():
        tacc[...] = jnp.full_like(tacc, -1e30)

        def one(b, s, m, qt, masked):
            cols = pl.ds(pl.multiple_of(qt * 256, 256), 256)
            r = s * 2 + m
            sc = jnp.dot(kscr[b], qz[r, :, cols], preferred_element_type=F32)
            if masked:
                k = lax.broadcasted_iota(jnp.int32, (1024, 256), 0)
                q = lax.broadcasted_iota(jnp.int32, (1024, 256), 1) + qt * 256
                sc = jnp.where(k <= q, sc, -1e30)
            tacc[r, :, cols] = jnp.maximum(
                tacc[r, :, cols], jnp.max(sc.reshape(128, 8, 256), axis=0)
            )

        @pl.loop(0, 8)
        def _(i):
            one(0, y, i // 4, lax.rem(i, 4), True)

        @pl.loop(0, full * 8)
        def _(i):
            b, s = which(i // 8)
            one(b, s, lax.rem(i // 4, 2), lax.rem(i, 4), False)

        for r in range(8):
            mref[r] = jnp.broadcast_to(jnp.max(tacc[r], axis=0, keepdims=True), (8, 1024))

    @pl.loop(0, 2)
    def _(attempt):
        @pl.when(flag[0] == 1)
        def _():
            @pl.when(attempt == 1)
            def _():
                tops()

            oacc[...] = jnp.zeros_like(oacc)
            tacc[...] = jnp.zeros_like(tacc)
            diagonal()

            @pl.when(full > 0)
            def _():
                b, s = which(jnp.int32(0))
                sbuf[0] = score(b, s, 0, 0)
                pl.loop(0, full)(pair)

            bad = jnp.int32(0)
            for s in range(4):
                has = jnp.logical_or(z > 0, y <= s)
                t = jnp.sum(tacc[2 * s : 2 * s + 2], axis=1)
                good = jnp.logical_and(
                    jnp.max(t) < BIG,
                    jnp.logical_or(jnp.min(t) > 1.0 / BIG, jnp.logical_not(has)),
                )
                bad = jnp.where(good, bad, 1)
            flag[0] = jnp.where(attempt == 0, bad, 0)

    for s, ref in enumerate((own, s1, s2, s3)):
        r = ysrc[s] * 2
        t0 = jnp.sum(tacc[r], axis=0, keepdims=True)
        t1 = jnp.sum(tacc[r + 1], axis=0, keepdims=True)
        m0 = mref[r, 0:1, :]
        m1 = mref[r + 1, 0:1, :]
        if s == 0:
            own[0] = oacc[r]
            own[1] = oacc[r + 1]
            stats[...] = jnp.concatenate([t0, t1, m0, m1, jnp.zeros((4, 1024), F32)], axis=0)
        else:
            ref[0:128, :] = oacc[r].astype(BF)
            ref[128:256, :] = oacc[r + 1].astype(BF)
            extra = split3(t0) + split3(t1) + split3(m0) + split3(m1) + [jnp.zeros((4, 1024), F32)]
            ref[256:272, :] = jnp.concatenate(extra, axis=0).astype(BF)


def attend(pos, qs, kvs):
    sent = jax.ShapeDtypeStruct((272, 1024), BF)
    return pl.pallas_call(
        attend_kernel,
        out_shape=(
            sent,
            sent,
            sent,
            jax.ShapeDtypeStruct((2, 128, 1024), F32),
            jax.ShapeDtypeStruct((8, 1024), F32),
        ),
        in_specs=[smem()] + [vmem()] * 8,
        out_specs=(vmem(),) * 5,
        scratch_shapes=[
            pltpu.VMEM((8, 128, 1024), BF),
            pltpu.VMEM((4, 1024, 128), BF),
            pltpu.VMEM((4, 128, 1024), BF),
            pltpu.VMEM((2, 1024, 256), F32),
            pltpu.VMEM((2, 1024, 256), BF),
            pltpu.VMEM((8, 128, 1024), F32),
            pltpu.VMEM((8, 8, 1024), F32),
            pltpu.VMEM((8, 8, 1024), F32),
            pltpu.SMEM((1,), jnp.int32),
        ],
        compiler_params=pltpu.CompilerParams(vmem_limit_bytes=40 * 1024 * 1024),
        cost_estimate=pl.CostEstimate(
            flops=12000000000, bytes_accessed=8000000, transcendentals=30000000
        ),
        name="attend",
    )(pos, *qs, *kvs)


def merge_kernel(pos, lam, own, stats, r1, r2, r3, gain, mine, other, lmine, lother):
    c = pos[2]
    mix = jnp.where(c == 0, lam[0], lam[1])

    def joined(ref, row):
        part = ref[256:272, :].astype(F32)
        return part[row : row + 1] + part[row + 1 : row + 2] + part[row + 2 : row + 3]

    heads = []
    logs = []
    for m in range(2):
        ts = [stats[m : m + 1, :]] + [joined(r, 3 * m) for r in (r1, r2, r3)]
        ms = [stats[2 + m : 3 + m, :]] + [joined(r, 6 + 3 * m) for r in (r1, r2, r3)]
        ms = [jnp.where(t > 0, v, -1e30) for t, v in zip(ts, ms)]
        top = jnp.maximum(jnp.maximum(ms[0], ms[1]), jnp.maximum(ms[2], ms[3]))
        ws = [jnp.exp2(v - top) for v in ms]
        total = ws[0] * ts[0] + ws[1] * ts[1] + ws[2] * ts[2] + ws[3] * ts[3]
        inv = 1.0 / total
        acc = own[m] * (ws[0] * inv)
        for w, r in zip(ws[1:], (r1, r2, r3)):
            acc = acc + r[m * 128 : (m + 1) * 128, :].astype(F32) * (w * inv)
        heads.append(acc)
        logs.append(top * math.log(2.0) + jnp.log(total))
    h = heads[0] - mix * heads[1]
    h = h * lax.rsqrt(jnp.mean(h * h, axis=0, keepdims=True) + 1e-06) * gain[...]
    lt = jnp.concatenate(logs, axis=0)
    a, b = h[:, :512], h[:, 512:]
    mine[...] = jnp.where(c == 0, a, b).T.astype(BF)
    other[...] = jnp.where(c == 0, b, a).T.astype(BF)
    lmine[...] = jnp.where(c == 0, lt[:, :512], lt[:, 512:])
    lother[...] = jnp.where(c == 0, lt[:, 512:], lt[:, :512])


def merge(pos, lam, own, stats, parts, gain):
    return pl.pallas_call(
        merge_kernel,
        out_shape=(
            jax.ShapeDtypeStruct((512, 128), BF),
            jax.ShapeDtypeStruct((512, 128), BF),
            jax.ShapeDtypeStruct((2, 512), F32),
            jax.ShapeDtypeStruct((2, 512), F32),
        ),
        in_specs=[smem(), smem()] + [vmem()] * 6,
        out_specs=(vmem(),) * 4,
        compiler_params=pltpu.CompilerParams(vmem_limit_bytes=24 * 1024 * 1024),
        cost_estimate=pl.CostEstimate(flops=500000000, bytes_accessed=4000000, transcendentals=0),
        name="merge",
    )(pos, lam, own, stats, *parts, gain)


def output_kernel(pos, moved, params, w, out, lhs):
    c = pos[2]
    total = jnp.zeros((128, 1), F32)
    square = jnp.zeros((128, 1), F32)
    for x in range(4):
        v = moved[x, :, 256:512].astype(F32)
        total = total + jnp.sum(v, axis=1, keepdims=True)
        square = square + jnp.sum(v * v, axis=1, keepdims=True)
        a = moved[x, :, 0:128]
        b = moved[x, :, 128:256]
        lhs[:, x * 256 : x * 256 + 128] = jnp.where(c == 0, a, b)
        lhs[:, x * 256 + 128 : x * 256 + 256] = jnp.where(c == 0, b, a)
    middle = total * (1.0 / 1024)
    inv = lax.rsqrt(square * (1.0 / 1024) - middle * middle + 1e-05)
    for x in range(4):
        v = moved[x, :, 256:512].astype(F32)
        v = (v - middle) * inv * params[x, 0:1, :] + params[x, 1:2, :]
        lhs[:, 1024 + x * 256 : 1280 + x * 256] = (v * jax.nn.sigmoid(v)).astype(BF)
    for i in range(4):
        cols = slice(i * 512, (i + 1) * 512)
        out[:, cols] = jnp.dot(lhs[...], w[:, cols], preferred_element_type=F32).astype(BF)


def output(pos, moved, params, w):
    return pl.pallas_call(
        output_kernel,
        out_shape=jax.ShapeDtypeStruct((128, 2048), BF),
        in_specs=[smem()] + [vmem()] * 3,
        out_specs=vmem(),
        scratch_shapes=[pltpu.VMEM((128, 2048), BF)],
        compiler_params=pltpu.CompilerParams(vmem_limit_bytes=24 * 1024 * 1024),
        cost_estimate=pl.CostEstimate(flops=1100000000, bytes_accessed=9000000, transcendentals=0),
        name="output",
    )(pos, moved, params, w)


def per_device(
    tokens, norm_gain, query_weight, key_weight, value_weight, glu_value_weight, glu_gate_weight,
    qk_gain, mix_lambda, head_gain, conv_kernel, channel_gain, channel_shift, output_weight,
):
    sp = lax.axis_index("sp").astype(jnp.int32)
    tp = lax.axis_index("tp").astype(jnp.int32)
    core = sp % NC
    pos = jnp.stack([sp // (NY * NC), (sp // NC) % NY, core, tp])
    t3 = along_x(tokens, 2)
    t1 = along_x(tokens, 1)
    t2 = along_x(tokens, -1)
    params = lax.all_gather(jnp.stack([channel_gain, channel_shift]), "tp", axis=0)
    place = (sp * 512 + jnp.arange(512, dtype=jnp.int32)).astype(F32)
    inverse = 10000.0 ** (-jnp.arange(0, 32, dtype=F32) * 2.0 / 64)
    angles = place[:, None] * inverse[None, :]
    cosine = jnp.cos(angles)
    sine = jnp.sin(angles)
    cos = jnp.concatenate([cosine] * 4, axis=1)
    sin = jnp.concatenate([-sine, sine, -sine, sine], axis=1)
    qkg = jnp.tile(qk_gain.reshape(1, 128), (1, 2))
    mine, other, gated = project(
        pos,
        (tokens, t1, t2, t3),
        norm_gain[None, :],
        (query_weight, key_weight, value_weight, glu_value_weight, glu_gate_weight),
        qkg,
        cos,
        sin,
    )
    theirs = to_sibling(other)
    halo = lax.ppermute(gated[512 - 30 :], "sp", [(i, i + 1) for i in range(31)])
    both = jnp.where(
        core == 0,
        jnp.concatenate([mine, theirs], axis=1),
        jnp.concatenate([theirs, mine], axis=1),
    )
    q = both[:128]
    kv = both[128:]
    kv1 = up_z(kv, 1)
    kv2 = up_z(kv, 2)
    kv3 = up_z(kv, 3)
    q1 = along_y(q, 1)
    q2 = along_y(q, -1)
    q3 = along_y(q, 2)
    conv = convolve(gated, halo, conv_kernel)
    o1, o2, o3, own, stats = attend(pos, (q, q1, q2, q3), (kv, kv1, kv2, kv3))
    back = (along_y(o1, -1), along_y(o2, 1), along_y(o3, 2))
    amine, aother, lmine, lother = merge(
        pos, mix_lambda, own, stats, back, head_gain[:, None]
    )
    atheirs = to_sibling(aother)
    ltheirs = to_sibling(lother)
    log_totals = jnp.where(
        core == 0, jnp.stack([lmine, ltheirs], axis=1), jnp.stack([ltheirs, lmine], axis=1)
    )
    merged = jnp.concatenate([amine, atheirs, conv], axis=1).reshape(4, 128, 512)
    moved = lax.all_to_all(merged, "tp", split_axis=0, concat_axis=0, tiled=True)
    mixed = output(pos, moved, params, output_weight)
    return (mixed, log_totals)


def solution(mesh):
    placed = (
        P(("sp", "tp"), None),
        P(),
        P(None, "tp"),
        P(None, "tp"),
        P(None, "tp"),
        P(None, "tp"),
        P(None, "tp"),
        P(),
        P("tp"),
        P(),
        P(None, "tp"),
        P("tp"),
        P("tp"),
        P(),
    )
    return jax.shard_map(
        per_device,
        mesh=mesh,
        in_specs=placed,
        out_specs=(P(("sp", "tp"), None), P(None, "tp", "sp")),
        check_vma=False,
    )
```

```python
import math

import jax
import jax.numpy as jnp
from jax import lax
from jax.experimental import pallas as pl
from jax.experimental.pallas import tpu as pltpu
from jax.sharding import PartitionSpec as P

NZ, NY, NC = 4, 4, 2
BIG = 2.0**100
LOG2E = math.log2(math.e)
BF = jnp.bfloat16
F32 = jnp.float32


def vmem():
    return pl.BlockSpec(memory_space=pltpu.VMEM)


def smem():
    return pl.BlockSpec(memory_space=pltpu.SMEM)


def moves(target):
    out = []
    for z in range(NZ):
        for y in range(NY):
            for c in range(NC):
                t = target(z, y, c)
                if t is not None:
                    out.append(((z * NY + y) * NC + c, (t[0] * NY + t[1]) * NC + t[2]))
    return out


def reads_query(z, y, c, qz, qy):
    return (z > 0 or qy > y) if c == 0 else qz > z


def reads_keys(z, y, c, kz, ky):
    return kz < z if c == 0 else (z < NZ - 1 or ky < y)


def stepped(z, y, along_y, step):
    return (z, (y + step) % NY) if along_y else ((z + step) % NZ, y)


def send_query(value, step):
    def target(z, y, c):
        t = stepped(z, y, c == 0, step)
        return (*t, c) if reads_query(*t, c, z, y) else None

    return lax.ppermute(value, "sp", moves(target))


def return_sum(value, step):
    def target(z, y, c):
        t = stepped(z, y, c == 0, -step)
        return (*t, c) if reads_query(z, y, c, *t) else None

    return lax.ppermute(value, "sp", moves(target))


def send_keys(value, step):
    def target(z, y, c):
        t = stepped(z, y, c == 1, step)
        return (*t, c) if reads_keys(*t, c, z, y) else None

    return lax.ppermute(value, "sp", moves(target))


def to_sibling(value):
    return lax.ppermute(value, "sp", moves(lambda z, y, c: (z, y, 1 - c)))


def along_x(value, step):
    count = lax.axis_size("tp")
    return lax.ppermute(value, "tp", [(i, (i + step) % count) for i in range(count)])


def hbm():
    return pl.BlockSpec(memory_space=pl.ANY)


def prefetch_kernel(*refs):
    n = (len(refs) - 1) // 2
    copies = [
        pltpu.make_async_copy(refs[i], refs[n + i], refs[2 * n].at[i]) for i in range(n)
    ]
    for copy in copies:
        copy.start()
    for copy in copies:
        copy.wait()


def prefetch(arrays):
    return pl.pallas_call(
        prefetch_kernel,
        out_shape=tuple(jax.ShapeDtypeStruct(a.shape, a.dtype) for a in arrays),
        in_specs=[hbm()] * len(arrays),
        out_specs=(vmem(),) * len(arrays),
        scratch_shapes=[pltpu.SemaphoreType.DMA((len(arrays),))],
        compiler_params=pltpu.CompilerParams(vmem_limit_bytes=48 * 1024 * 1024),
        cost_estimate=pl.CostEstimate(flops=2000000, bytes_accessed=12000000, transcendentals=0),
        name="prefetch",
    )(*arrays)


def project_body(pos, pieces, gain, ws, qkg, cos, sin, mine, other, normed):
    x = pos[3]
    c = pos[2]
    ats = []
    row = 0
    for ref, step in pieces:
        t = ref[...].astype(F32)
        n = t.shape[0]
        ms = jnp.mean(t * t, axis=-1, keepdims=True)
        normed[row : row + n, :] = (t * lax.rsqrt(ms + 1e-06) * gain[...]).astype(BF)
        if row % 128 == 0:
            ats.append(pl.multiple_of(lax.rem(x + step, 4) * 128, 128))
        row += n
    lane = lax.broadcasted_iota(jnp.int32, (1, 256), 1)
    first = lax.rem(lane, 64) < 32
    gi = lax.broadcasted_iota(jnp.int32, (256, 256), 0) // 64
    gj = lax.broadcasted_iota(jnp.int32, (256, 256), 1) // 64
    groups = jnp.where(gi == gj, 1.0 / 64, 0.0).astype(BF)

    def table(ref):
        v = jnp.concatenate([ref[pl.ds(at, 128), :] for at in ats], axis=0)
        return jnp.concatenate([v, v], axis=1)

    cc = table(cos)
    ss = table(sin)

    def times(w):
        return jnp.dot(normed[...], w[...], preferred_element_type=F32).astype(BF).astype(F32)

    def turned(w):
        v = times(w)
        sq = v * v
        hi = sq.astype(BF)
        lo = (sq - hi.astype(F32)).astype(BF)
        ms = jnp.dot(hi, groups, preferred_element_type=F32) + jnp.dot(
            lo, groups, preferred_element_type=F32
        )
        v = v * lax.rsqrt(ms + 1e-06) * qkg[...]
        swapped = jnp.where(first, pltpu.roll(v, 256 - 32, 1), pltpu.roll(v, 32, 1))
        return v * cc + swapped * ss

    def put(row, v, flip):
        a = v[:, :128]
        b = v[:, 128:]
        for ref, val in ((mine, jnp.where(c == 0, a, b)), (other, jnp.where(c == 0, b, a))):
            for i, at in enumerate(ats):
                part = val[i * 128 : (i + 1) * 128, :]
                ref[row : row + 128, pl.ds(at, 128)] = (part.T if flip else part).astype(BF)

    wq, wk, wv, wa, wg = ws
    put(0, turned(wq) * (LOG2E / 8.0), True)
    put(128, turned(wk), False)
    put(256, times(wv), True)
    g = times(wa) * jax.nn.sigmoid(times(wg))
    put(384, g, False)


def project_first(pos, t0, t1, t2, gain, wq, wk, wv, wa, wg, qkg, cos, sin, mine, other, normed):
    project_body(
        pos, ((t0, 0), (t1, 3), (t2, 1)), gain, (wq, wk, wv, wa, wg), qkg, cos, sin,
        mine, other, normed,
    )


def project_last(
    pos, t3, t4, gain, wq, wk, wv, wa, wg, qkg, cos, sin, mine_in, other_in, mine, other, normed
):
    project_body(
        pos, ((t3, 2), (t4, 2)), gain, (wq, wk, wv, wa, wg), qkg, cos, sin,
        mine, other, normed,
    )


def project(body, rows, pos, pieces, shared, filled):
    count = 1 + len(pieces) + len(shared) + len(filled)
    start = count - len(filled)
    return pl.pallas_call(
        body,
        out_shape=(
            jax.ShapeDtypeStruct((512, 512), BF),
            jax.ShapeDtypeStruct((512, 512), BF),
        ),
        in_specs=[smem()] + [vmem()] * (count - 1),
        out_specs=(vmem(),) * 2,
        scratch_shapes=[pltpu.VMEM((rows, 2048), BF)],
        input_output_aliases={start + i: i for i in range(len(filled))},
        compiler_params=pltpu.CompilerParams(vmem_limit_bytes=14 * 1024 * 1024),
        cost_estimate=pl.CostEstimate(
            flops=5242880 * rows, bytes_accessed=8000000, transcendentals=0
        ),
    )(pos, *pieces, *shared, *filled)


def conv_kernel_body(pos, gated, halo, taps, out, ext):
    w = jnp.where(pos[2] == 0, taps[:, :128], taps[:, 128:])
    ext[0:32, :] = jnp.zeros((32, 128), F32)
    ext[1056:1072, :] = jnp.zeros((16, 128), F32)
    ext[2:32, :] = halo[...].astype(F32)
    for i in range(8):
        ext[32 + i * 128 : 160 + i * 128, :] = gated[:, i * 128 : (i + 1) * 128].astype(F32)
    for i in range(8):
        acc = jnp.zeros((128, 128), F32)
        for r in range(8):
            moved = ext[i * 128 + r : i * 128 + r + 160, :]
            for a in range(5):
                j = a * 8 + r - 2
                if 0 <= j < 31:
                    acc = acc + w[j : j + 1, :] * moved[8 * a : 8 * a + 128]
        out[i] = acc.astype(BF)


def convolve(pos, gated, halo, taps):
    return pl.pallas_call(
        conv_kernel_body,
        out_shape=jax.ShapeDtypeStruct((8, 128, 128), BF),
        in_specs=[smem()] + [vmem()] * 3,
        out_specs=vmem(),
        scratch_shapes=[pltpu.VMEM((1072, 128), F32)],
        compiler_params=pltpu.CompilerParams(vmem_limit_bytes=4 * 1024 * 1024),
        cost_estimate=pl.CostEstimate(flops=1000000000, bytes_accessed=800000, transcendentals=0),
        name="convolve",
    )(pos, gated, halo, taps)


def split3(v):
    hi = v.astype(BF).astype(F32)
    mid = (v - hi).astype(BF).astype(F32)
    return [hi, mid, v - hi - mid]


ITEMS = [(m, qt) for m in range(2) for qt in range(4)]


def chips(pos):
    z, y, c = pos[0], pos[1], pos[2]
    own = z * 4 + y
    over_y = [own] + [z * 4 + lax.rem(y + d, 4) for d in (3, 1, 2)]
    over_z = [own] + [lax.rem(z + d, 4) * 4 + y for d in (3, 1, 2)]
    queries = [jnp.where(c == 0, a, b) for a, b in zip(over_y, over_z)]
    keys = [jnp.where(c == 0, b, a) for a, b in zip(over_y, over_z)]
    return queries, keys


def load_query(ref, qz, i):
    rows = lax.broadcasted_iota(jnp.int32, (128, 1024), 0)
    q = ref[...]
    qz[2 * i] = jnp.where(rows < 64, q, jnp.zeros_like(q))
    qz[2 * i + 1] = jnp.where(rows >= 64, q, jnp.zeros_like(q))


def load_keys(ref, kscr, vscr, b):
    for i in range(8):
        kscr[b, i * 128 : (i + 1) * 128, :] = ref[0:128, i * 128 : (i + 1) * 128]
    vscr[b] = ref[128:256, :]


def list_pairs(todo, pairs, queries, keys):
    n = jnp.int32(0)
    todo[0] = 0
    for i, s, b in pairs:
        ok = keys[b] < queries[s]

        @pl.when(ok)
        def _(n=n, i=i, b=b):
            todo[n] = i * 4 + b
            todo[n + 1] = i * 4 + b

        n = n + ok.astype(jnp.int32)
    return n


def weigh(tacc, mref, r, cols, scores, masked):
    n = scores.shape[0]
    s3 = scores.reshape(n // 8, 8, 256)
    if mref is not None:
        s3 = s3 - mref[r, :, cols][None]
    p = jnp.exp2(s3).reshape(n, 256)
    if masked:
        k = lax.broadcasted_iota(jnp.int32, (256, 256), 0)
        q = lax.broadcasted_iota(jnp.int32, (256, 256), 1)
        last = jnp.where(k <= q, p[n - 256 :], 0.0)
        p = last if n == 256 else jnp.concatenate([p[: n - 256], last], axis=0)
    tacc[r, :, cols] += jnp.sum(p.reshape(n // 8, 8, 256), axis=0)
    return p.astype(BF)


def run_pairs(todo, n, qz, kscr, vscr, sbuf, pbuf, oacc, tacc, mref):
    def score(e, m, qt):
        return jnp.dot(
            kscr[e & 3],
            qz[(e >> 2) * 2 + m, :, qt * 256 : (qt + 1) * 256],
            preferred_element_type=F32,
        )

    @pl.when(n > 0)
    def _():
        sbuf[0] = score(todo[0], 0, 0)

        @pl.loop(0, n)
        def _(t):
            e = todo[t]
            later = todo[t + 1]
            for i, (m, qt) in enumerate(ITEMS):
                if i + 1 < len(ITEMS):
                    sbuf[(i + 1) % 2] = score(e, *ITEMS[i + 1])
                else:
                    sbuf[0] = score(later, 0, 0)
                cols = slice(qt * 256, (qt + 1) * 256)
                r = (e >> 2) * 2 + m
                pbuf[i % 2] = weigh(tacc, mref, r, cols, sbuf[i % 2], False)
                oacc[r, :, cols] += jnp.dot(vscr[e & 3], pbuf[i % 2], preferred_element_type=F32)


def run_diagonal(qz, kscr, vscr, sbuf, pbuf, oacc, tacc, mref):
    for i, (m, qt) in enumerate(ITEMS):
        n = (qt + 1) * 256
        cols = slice(qt * 256, n)
        sbuf[i % 2, :n, :] = jnp.dot(kscr[0, :n, :], qz[m, :, cols], preferred_element_type=F32)
        pbuf[i % 2, :n, :] = weigh(tacc, mref, m, cols, sbuf[i % 2, :n, :], True)
        oacc[m, :, cols] += jnp.dot(vscr[0, :, :n], pbuf[i % 2, :n, :], preferred_element_type=F32)


def take_tops(todo, n, own, qz, kscr, tacc, mref):
    tacc[...] = jnp.full_like(tacc, -1e30)

    def one(b, r, qt, masked):
        cols = pl.ds(pl.multiple_of(qt * 256, 256), 256)
        sc = jnp.dot(kscr[b], qz[r, :, cols], preferred_element_type=F32)
        if masked:
            k = lax.broadcasted_iota(jnp.int32, (1024, 256), 0)
            q = lax.broadcasted_iota(jnp.int32, (1024, 256), 1) + qt * 256
            sc = jnp.where(k <= q, sc, -1e30)
        tacc[r, :, cols] = jnp.maximum(tacc[r, :, cols], jnp.max(sc.reshape(128, 8, 256), axis=0))

    if own:

        @pl.loop(0, 8)
        def _(i):
            one(0, i >> 2, i & 3, True)

    @pl.loop(0, n * 8)
    def _(i):
        e = todo[i >> 3]
        one(e & 3, (e >> 2) * 2 + ((i >> 2) & 1), i & 3, False)

    for r in range(mref.shape[0]):
        mref[r] = jnp.broadcast_to(jnp.max(tacc[r], axis=0, keepdims=True), (8, 1024))


def finish(sources, fast, pos, qz, kvs, kscr, vscr, sbuf, pbuf, oacc, tacc, mref, todo, flag):
    queries, keys = chips(pos)
    mref[...] = jnp.zeros_like(mref)
    flag[0] = 1

    @pl.loop(0, 2)
    def _(attempt):
        @pl.when(flag[0] == 1)
        def _():
            flag[1] = list_pairs(todo, fast, queries, keys)

            @pl.when(attempt == 1)
            def _():
                for b in range(4):
                    load_keys(kvs[b], kscr, vscr, b)
                every = [(i, s, b) for i, s in enumerate(sources) for b in range(4)]
                flag[1] = list_pairs(todo, every, queries, keys)
                take_tops(todo, flag[1], 0 in sources, qz, kscr, tacc, mref)
                oacc[...] = jnp.zeros_like(oacc)
                tacc[...] = jnp.zeros_like(tacc)
                if 0 in sources:
                    run_diagonal(qz, kscr, vscr, sbuf, pbuf, oacc, tacc, mref)

            run_pairs(todo, flag[1], qz, kscr, vscr, sbuf, pbuf, oacc, tacc, mref)
            worst = jnp.zeros((1, 1024), F32)
            for i, s in enumerate(sources):
                has = s == 0
                for b in range(4):
                    has = jnp.logical_or(has, keys[b] < queries[s])
                least = jnp.where(has, 1.0 / BIG, -1.0)
                for m in range(2):
                    t = jnp.sum(tacc[2 * i + m], axis=0, keepdims=True)
                    good = jnp.logical_and(t < BIG, t > least)
                    worst = jnp.where(good, worst, 1.0)
            bad = (jnp.max(worst) > 0.5).astype(jnp.int32)
            flag[0] = jnp.where(attempt == 0, bad, 0)


def write_sum(ref, i, oacc, tacc, mref):
    r = 2 * i
    t = [jnp.sum(tacc[r + m], axis=0, keepdims=True) for m in range(2)]
    ref[0:128, :] = oacc[r].astype(BF)
    ref[128:256, :] = oacc[r + 1].astype(BF)
    extra = split3(t[0]) + split3(t[1])
    extra = extra + split3(mref[r, 0:1, :]) + split3(mref[r + 1, 0:1, :])
    ref[256:272, :] = jnp.concatenate(extra + [jnp.zeros((4, 1024), F32)], axis=0).astype(BF)


def near_kernel(pos, q0, q1, q2, kv0, kv1, kv2, oacc, tacc, qz, kscr, vscr, sbuf, pbuf, todo):
    queries, keys = chips(pos)
    for i, ref in enumerate((q0, q1, q2)):
        load_query(ref, qz, i)
    for b, ref in enumerate((kv0, kv1, kv2)):
        load_keys(ref, kscr, vscr, b)
    oacc[...] = jnp.zeros_like(oacc)
    tacc[...] = jnp.zeros_like(tacc)
    n = list_pairs(todo, [(s, s, b) for b in range(3) for s in range(3)], queries, keys)
    run_diagonal(qz, kscr, vscr, sbuf, pbuf, oacc, tacc, None)
    run_pairs(todo, n, qz, kscr, vscr, sbuf, pbuf, oacc, tacc, None)


def far_kernel(
    pos, q3, kv0, kv1, kv2, kv3, near, out, token, qz, kscr, vscr, sbuf, pbuf, oacc, tacc, mref, todo, flag
):
    load_query(q3, qz, 0)
    kvs = (kv0, kv1, kv2, kv3)
    for b in range(4):
        load_keys(kvs[b], kscr, vscr, b)
    oacc[...] = jnp.zeros_like(oacc)
    tacc[...] = jnp.zeros_like(tacc)
    fast = [(0, 3, b) for b in range(4)]
    finish((3,), fast, pos, qz, kvs, kscr, vscr, sbuf, pbuf, oacc, tacc, mref, todo, flag)
    write_sum(out, 0, oacc, tacc, mref)
    token[...] = jnp.zeros_like(token)


def last_kernel(
    pos, q0, q1, q2, kv0, kv1, kv2, kv3, oin, tin, token, oacc, tacc, out1, out2, stats,
    qz, kscr, vscr, sbuf, pbuf, mref, todo, flag,
):
    for i, ref in enumerate((q0, q1, q2)):
        load_query(ref, qz, i)
    kvs = (kv0, kv1, kv2, kv3)
    load_keys(kv3, kscr, vscr, 3)
    fast = [(s, s, 3) for s in range(3)]
    finish((0, 1, 2), fast, pos, qz, kvs, kscr, vscr, sbuf, pbuf, oacc, tacc, mref, todo, flag)
    write_sum(out1, 1, oacc, tacc, mref)
    write_sum(out2, 2, oacc, tacc, mref)
    t = [jnp.sum(tacc[m], axis=0, keepdims=True) for m in range(2)]
    stats[...] = jnp.concatenate(
        t + [mref[0, 0:1, :], mref[1, 0:1, :], jnp.zeros((4, 1024), F32)], axis=0
    )


def scratch(queries, blocks, extra):
    return [
        pltpu.VMEM((2 * queries, 128, 1024), BF),
        pltpu.VMEM((blocks, 1024, 128), BF),
        pltpu.VMEM((blocks, 128, 1024), BF),
        pltpu.VMEM((2, 1024, 256), F32),
        pltpu.VMEM((2, 1024, 256), BF),
        *extra,
        pltpu.SMEM((20,), jnp.int32),
    ]


def attention_call(body, ins, outs, scratches, pairs, aliases=None):
    return pl.pallas_call(
        body,
        out_shape=outs,
        in_specs=[smem()] + [vmem()] * (len(ins) - 1),
        out_specs=(vmem(),) * len(outs),
        scratch_shapes=scratches,
        input_output_aliases=aliases or {},
        compiler_params=pltpu.CompilerParams(vmem_limit_bytes=12 * 1024 * 1024),
        cost_estimate=pl.CostEstimate(
            flops=800000000 * pairs, bytes_accessed=4000000, transcendentals=2000000 * pairs
        ),
    )(*ins)


def attend_near(pos, qs, kvs):
    outs = (
        jax.ShapeDtypeStruct((6, 128, 1024), F32),
        jax.ShapeDtypeStruct((6, 8, 1024), F32),
    )
    ins = (pos, *qs, *kvs)
    return attention_call(near_kernel, ins, outs, scratch(3, 3, []), 8)


def attend_far(pos, q, kvs, near):
    outs = (jax.ShapeDtypeStruct((272, 1024), BF), jax.ShapeDtypeStruct((8, 128), F32))
    extra = [
        pltpu.VMEM((2, 128, 1024), F32),
        pltpu.VMEM((2, 8, 1024), F32),
        pltpu.VMEM((2, 8, 1024), F32),
    ]
    return attention_call(
        far_kernel,
        (pos, q, *kvs, near),
        outs,
        scratch(1, 4, extra) + [pltpu.SMEM((2,), jnp.int32)],
        4,
    )


def attend_last(pos, qs, kvs, oacc, tacc, token):
    sent = jax.ShapeDtypeStruct((272, 1024), BF)
    outs = (
        jax.ShapeDtypeStruct((6, 128, 1024), F32),
        jax.ShapeDtypeStruct((6, 8, 1024), F32),
        sent,
        sent,
        jax.ShapeDtypeStruct((8, 1024), F32),
    )
    ins = (pos, *qs, *kvs, oacc, tacc, token)
    extra = [pltpu.VMEM((6, 8, 1024), F32)]
    return attention_call(
        last_kernel,
        ins,
        outs,
        scratch(3, 4, extra) + [pltpu.SMEM((2,), jnp.int32)],
        3,
        {8: 0, 9: 1},
    )


def merge_kernel(pos, lam, own, stats, r1, r2, r3, gain, conv, scale, shift, packed, lmine, lother):
    c = pos[2]
    mix = jnp.where(c == 0, lam[0], lam[1])

    def joined(ref, row):
        part = ref[256:272, :].astype(F32)
        return part[row : row + 1] + part[row + 1 : row + 2] + part[row + 2 : row + 3]

    heads = []
    logs = []
    for m in range(2):
        ts = [stats[m : m + 1, :]] + [joined(r, 3 * m) for r in (r1, r2, r3)]
        ms = [stats[2 + m : 3 + m, :]] + [joined(r, 6 + 3 * m) for r in (r1, r2, r3)]
        ms = [jnp.where(t > 0, v, -1e30) for t, v in zip(ts, ms)]
        top = jnp.maximum(jnp.maximum(ms[0], ms[1]), jnp.maximum(ms[2], ms[3]))
        ws = [jnp.exp2(v - top) for v in ms]
        total = ws[0] * ts[0] + ws[1] * ts[1] + ws[2] * ts[2] + ws[3] * ts[3]
        inv = 1.0 / total
        acc = own[m] * (ws[0] * inv)
        for w, r in zip(ws[1:], (r1, r2, r3)):
            acc = acc + r[m * 128 : (m + 1) * 128, :].astype(F32) * (w * inv)
        heads.append(acc)
        logs.append(top * math.log(2.0) + jnp.log(total))
    h = heads[0] - mix * heads[1]
    h = h * lax.rsqrt(jnp.mean(h * h, axis=0, keepdims=True) + 1e-06)
    lt = jnp.concatenate(logs, axis=0)
    sc = jnp.where(c == 0, scale[:, :128], scale[:, 128:])
    sh = jnp.where(c == 0, shift[:, :128], shift[:, 128:])
    extra = jnp.concatenate(split3(sc) + split3(sh) + [jnp.zeros((10, 128), F32)], axis=0)
    extra = jnp.concatenate([jnp.zeros((16, 128), F32), extra], axis=1).astype(BF)
    for i in range(8):
        packed[i, 128:144, :] = extra
        packed[i, 0:128, 0:128] = (h[:, i * 128 : (i + 1) * 128].T * gain[...]).astype(BF)
        packed[i, 0:128, 128:256] = conv[i]
    lmine[...] = jnp.where(c == 0, lt[:, :512], lt[:, 512:])
    lother[...] = jnp.where(c == 0, lt[:, 512:], lt[:, :512])


def merge(pos, lam, own, stats, parts, gain, conv, scale, shift):
    return pl.pallas_call(
        merge_kernel,
        out_shape=(
            jax.ShapeDtypeStruct((8, 144, 256), BF),
            jax.ShapeDtypeStruct((2, 512), F32),
            jax.ShapeDtypeStruct((2, 512), F32),
        ),
        in_specs=[smem(), smem()] + [vmem()] * 9,
        out_specs=(vmem(),) * 3,
        compiler_params=pltpu.CompilerParams(vmem_limit_bytes=8 * 1024 * 1024),
        cost_estimate=pl.CostEstimate(flops=500000000, bytes_accessed=4000000, transcendentals=0),
        name="merge",
    )(pos, lam, own, stats, *parts, gain, conv, scale, shift)


def output_kernel(moved, w, out, lhs, held, sem):
    copies = [
        pltpu.make_async_copy(w.at[:, i * 512 : (i + 1) * 512], held.at[i], sem.at[i])
        for i in range(4)
    ]
    for copy in copies:
        copy.start()
    total = jnp.zeros((128, 1), F32)
    square = jnp.zeros((128, 1), F32)
    for i in range(8):
        v = moved[i, 0:128, 128:256].astype(F32)
        total = total + jnp.sum(v, axis=1, keepdims=True)
        square = square + jnp.sum(v * v, axis=1, keepdims=True)
    middle = total * (1.0 / 1024)
    inv = lax.rsqrt(square * (1.0 / 1024) - middle * middle + 1e-05)
    for c in range(2):
        for k in range(4):
            at = k * 256 + c * 128
            p = moved[c * 4 + k, 128:144, 128:256].astype(F32)
            gain = p[0:1] + p[1:2] + p[2:3]
            shift = p[3:4] + p[4:5] + p[5:6]
            lhs[:, at : at + 128] = moved[c * 4 + k, 0:128, 0:128]
            v = moved[c * 4 + k, 0:128, 128:256].astype(F32)
            v = (v - middle) * inv * gain + shift
            lhs[:, 1024 + at : 1152 + at] = (v * jax.nn.sigmoid(v)).astype(BF)
    for i, copy in enumerate(copies):
        copy.wait()
        out[:, i * 512 : (i + 1) * 512] = jnp.dot(
            lhs[...], held[i], preferred_element_type=F32
        ).astype(BF)


def output(moved, w):
    return pl.pallas_call(
        output_kernel,
        out_shape=jax.ShapeDtypeStruct((128, 2048), BF),
        in_specs=[vmem(), pl.BlockSpec(memory_space=pltpu.HBM)],
        out_specs=vmem(),
        scratch_shapes=[
            pltpu.VMEM((128, 2048), BF),
            pltpu.VMEM((4, 2048, 512), BF),
            pltpu.SemaphoreType.DMA((4,)),
        ],
        compiler_params=pltpu.CompilerParams(vmem_limit_bytes=52 * 1024 * 1024),
        cost_estimate=pl.CostEstimate(flops=1100000000, bytes_accessed=9000000, transcendentals=0),
        name="output",
    )(moved, w)


def per_device_steps(
    tokens, norm_gain, query_weight, key_weight, value_weight, glu_value_weight, glu_gate_weight,
    qk_gain, mix_lambda, head_gain, conv_kernel, channel_gain, channel_shift, output_weight,
):
    sp = lax.axis_index("sp").astype(jnp.int32)
    tp = lax.axis_index("tp").astype(jnp.int32)
    core = sp % NC
    pos = jnp.stack([sp // (NY * NC), (sp // NC) % NY, core, tp])
    t1 = along_x(tokens, 1)
    t2 = along_x(tokens, -1)
    t3 = along_x(t1[:64], 1)
    t4 = along_x(t2[64:], -1)
    place = (sp * 512 + jnp.arange(512, dtype=jnp.int32)).astype(F32)
    inverse = 10000.0 ** (-jnp.arange(0, 32, dtype=F32) * 2.0 / 64)
    angles = place[:, None] * inverse[None, :]
    cosine = jnp.cos(angles)
    sine = jnp.sin(angles)
    cos = jnp.concatenate([cosine] * 4, axis=1)
    sin = jnp.concatenate([-sine, sine, -sine, sine], axis=1)
    qkg = jnp.tile(qk_gain.reshape(1, 128), (1, 2))
    t0, *weights = prefetch(
        (tokens, query_weight, key_weight, value_weight, glu_value_weight, glu_gate_weight)
    )
    shared = (
        norm_gain[None, :],
        *weights,
        qkg,
        cos,
        sin,
    )
    filled = project(project_first, 384, pos, (t0, t1, t2), shared, ())
    mine, other = project(project_last, 128, pos, (t3, t4), shared, filled)
    theirs = to_sibling(other)
    both = jnp.where(
        core == 0,
        jnp.concatenate([mine, theirs], axis=1),
        jnp.concatenate([theirs, mine], axis=1),
    )
    q = both[:128]
    kv = both[128:384]
    gated = both[384:]
    halo = lax.ppermute(gated[98:, 896:], "sp", [(i, i + NC) for i in range(NZ * NY * NC - NC)])
    q1 = send_query(q, 1)
    q2 = send_query(q, -1)
    kv1 = send_keys(kv, 1)
    kv2 = send_keys(kv, -1)
    q3 = send_query(q, 2)
    kv3 = send_keys(kv, 2)
    conv = convolve(pos, gated, halo, conv_kernel)
    oacc, tacc = attend_near(pos, (q, q1, q2), (kv, kv1, kv2))
    o3, token = attend_far(pos, q3, (kv, kv1, kv2, kv3), tacc)
    r3 = return_sum(o3, 2)
    own, _, o1, o2, stats = attend_last(pos, (q, q1, q2), (kv, kv1, kv2, kv3), oacc, tacc, token)
    r1 = return_sum(o1, 1)
    r2 = return_sum(o2, -1)
    packed, lmine, lother = merge(
        pos,
        mix_lambda,
        own,
        stats,
        (r1, r2, r3),
        head_gain[None, :],
        conv,
        channel_gain[None, :],
        channel_shift[None, :],
    )
    ltheirs = to_sibling(lother)
    log_totals = jnp.where(
        core == 0, jnp.stack([lmine, ltheirs], axis=1), jnp.stack([ltheirs, lmine], axis=1)
    )
    groups = [
        [(chip * NC + c) * 4 + x for c in range(NC) for x in range(4)] for chip in range(NZ * NY)
    ]
    moved = lax.all_to_all(
        packed, ("sp", "tp"), split_axis=0, concat_axis=0, axis_index_groups=groups, tiled=True
    )
    mixed = output(moved, output_weight)
    return (mixed, log_totals)


def solution(mesh):
    placed = (
        P(("sp", "tp"), None),
        P(),
        P(None, "tp"),
        P(None, "tp"),
        P(None, "tp"),
        P(None, "tp"),
        P(None, "tp"),
        P(),
        P("tp"),
        P(),
        P(None, "tp"),
        P("tp"),
        P("tp"),
        P(),
    )
    return jax.shard_map(
        per_device_steps,
        mesh=mesh,
        in_specs=placed,
        out_specs=(P(("sp", "tp"), None), P(None, "tp", "sp")),
        check_vma=False,
    )
```

```python
import math

import jax
import jax.numpy as jnp
from jax import lax
from jax.experimental import pallas as pl
from jax.experimental.pallas import tpu as pltpu
from jax.sharding import PartitionSpec as P

NZ, NY, NC = 4, 4, 2
BIG = 2.0**100
LOG2E = math.log2(math.e)
BF = jnp.bfloat16
F32 = jnp.float32


def vmem():
    return pl.BlockSpec(memory_space=pltpu.VMEM)


def smem():
    return pl.BlockSpec(memory_space=pltpu.SMEM)


def moves(target):
    out = []
    for z in range(NZ):
        for y in range(NY):
            for c in range(NC):
                t = target(z, y, c)
                if t is not None:
                    out.append(((z * NY + y) * NC + c, (t[0] * NY + t[1]) * NC + t[2]))
    return out


def stepped(z, y, along_y, step):
    return (z, (y + step) % NY) if along_y else ((z + step) % NZ, y)


def send_query(value, step):
    return lax.ppermute(
        value, "sp", moves(lambda z, y, c: (*stepped(z, y, c == 0, step), c))
    )


def send_keys(value, step):
    return lax.ppermute(
        value, "sp", moves(lambda z, y, c: (*stepped(z, y, c == 1, step), c))
    )


def to_mirror(value):
    return lax.ppermute(value, "sp", moves(lambda z, y, c: (NZ - 1 - z, y, 1 - c)))


def along_x(value, step):
    count = lax.axis_size("tp")
    return lax.ppermute(value, "tp", [(i, (i + step) % count) for i in range(count)])


def hbm():
    return pl.BlockSpec(memory_space=pl.ANY)


def prefetch_kernel(*refs):
    n = (len(refs) - 3) // 2
    copies = [
        pltpu.make_async_copy(refs[i], refs[n + 2 + i], refs[2 * n + 2].at[i]) for i in range(n)
    ]
    for copy in copies:
        copy.start()
    for copy in copies:
        copy.wait()


def prefetch(arrays, *tables):
    return pl.pallas_call(
        prefetch_kernel,
        out_shape=tuple(jax.ShapeDtypeStruct(a.shape, a.dtype) for a in arrays),
        in_specs=[hbm()] * len(arrays) + [vmem()] * 2,
        out_specs=(vmem(),) * len(arrays),
        scratch_shapes=[pltpu.SemaphoreType.DMA((len(arrays),))],
        compiler_params=pltpu.CompilerParams(vmem_limit_bytes=48 * 1024 * 1024),
        cost_estimate=pl.CostEstimate(flops=2000000, bytes_accessed=12000000, transcendentals=0),
        name="prefetch",
    )(*arrays, *tables)


def project_body(pos, pieces, gain, ws, qkg, cos, sin, mine, other, gated, normed):
    x = pos[3]
    c = pos[2]
    ats = []
    row = 0
    for ref, step in pieces:
        t = ref[...].astype(F32)
        n = t.shape[0]
        ms = jnp.mean(t * t, axis=-1, keepdims=True)
        normed[row : row + n, :] = (t * lax.rsqrt(ms + 1e-06) * gain[...]).astype(BF)
        if row % 128 == 0:
            ats.append(pl.multiple_of(lax.rem(x + step, 4) * 128, 128))
        row += n
    lane = lax.broadcasted_iota(jnp.int32, (1, 256), 1)
    first = lax.rem(lane, 64) < 32
    gi = lax.broadcasted_iota(jnp.int32, (256, 256), 0) // 64
    gj = lax.broadcasted_iota(jnp.int32, (256, 256), 1) // 64
    groups = jnp.where(gi == gj, 1.0 / 64, 0.0).astype(BF)

    def table(ref):
        v = jnp.concatenate([ref[pl.ds(at, 128), :] for at in ats], axis=0)
        return jnp.concatenate([v, v], axis=1)

    cc = table(cos)
    ss = table(sin)

    def times(w):
        return jnp.dot(normed[...], w[...], preferred_element_type=F32).astype(BF).astype(F32)

    def turned(w):
        v = times(w)
        sq = v * v
        hi = sq.astype(BF)
        lo = (sq - hi.astype(F32)).astype(BF)
        ms = jnp.dot(hi, groups, preferred_element_type=F32) + jnp.dot(
            lo, groups, preferred_element_type=F32
        )
        v = v * lax.rsqrt(ms + 1e-06) * qkg[...]
        swapped = jnp.where(first, pltpu.roll(v, 256 - 32, 1), pltpu.roll(v, 32, 1))
        return v * cc + swapped * ss

    def put(row, v, flip):
        a = v[:, :128]
        b = v[:, 128:]
        kept = jnp.where(c == 0, a, b)
        given = jnp.where(c == 0, b, a)
        for i, at in enumerate(ats):
            rows = slice(i * 128, (i + 1) * 128)
            part = kept[rows, :]
            mine[row : row + 128, pl.ds(at, 128)] = (part.T if flip else part).astype(BF)
            part = given[rows, :]
            other[row : row + 128, rows] = (part.T if flip else part).astype(BF)

    wq, wk, wv, wa, wg = ws
    put(0, turned(wq) * (LOG2E / 8.0), True)
    put(128, turned(wk), False)
    put(256, times(wv), True)
    g = times(wa) * jax.nn.sigmoid(times(wg))
    for i, at in enumerate(ats):
        gated[pl.ds(at, 128), :] = g[i * 128 : (i + 1) * 128, :].astype(BF)


def project_first(
    pos, t0, a1, b1, b2, a2, gain, wq, wk, wv, wa, wg, qkg, cos, sin, mine, gated, other, normed
):
    project_body(
        pos, ((t0, 0), (a1, 3), (b1, 3), (b2, 1), (a2, 1)), gain, (wq, wk, wv, wa, wg), qkg, cos,
        sin, mine, other, gated, normed,
    )


def project_last(
    pos, f1, f2, gain, wq, wk, wv, wa, wg, qkg, cos, sin, mine_in, gated_in, mine, gated, other,
    normed,
):
    project_body(
        pos, ((f1, 2), (f2, 2)), gain, (wq, wk, wv, wa, wg), qkg, cos, sin,
        mine, other, gated, normed,
    )


def project(body, rows, pos, pieces, shared, filled):
    count = 1 + len(pieces) + len(shared) + len(filled)
    start = count - len(filled)
    return pl.pallas_call(
        body,
        out_shape=(
            jax.ShapeDtypeStruct((384, 512), BF),
            jax.ShapeDtypeStruct((512, 256), BF),
            jax.ShapeDtypeStruct((384, rows), BF),
        ),
        in_specs=[smem()] + [vmem()] * (count - 1),
        out_specs=(vmem(),) * 3,
        scratch_shapes=[pltpu.VMEM((rows, 2048), BF)],
        input_output_aliases={start + i: i for i in range(len(filled))},
        compiler_params=pltpu.CompilerParams(vmem_limit_bytes=14 * 1024 * 1024),
        cost_estimate=pl.CostEstimate(
            flops=5242880 * rows, bytes_accessed=8000000, transcendentals=0
        ),
    )(pos, *pieces, *shared, *filled)


def assemble_kernel(pos, mine, near, far, q, kv):
    x = pos[3]
    q[:, 0:512] = mine[0:128, :]
    kv[:, 0:512] = mine[128:384, :]
    for i, step in enumerate((0, 3, 1, 2)):
        at = pl.multiple_of(512 + lax.rem(x + step, 4) * 128, 128)
        ref = near if i < 3 else far
        cols = slice(i * 128, (i + 1) * 128) if i < 3 else slice(0, 128)
        q[:, pl.ds(at, 128)] = ref[0:128, cols]
        kv[:, pl.ds(at, 128)] = ref[128:384, cols]


def assemble(pos, mine, near, far):
    return pl.pallas_call(
        assemble_kernel,
        out_shape=(
            jax.ShapeDtypeStruct((128, 1024), BF),
            jax.ShapeDtypeStruct((256, 1024), BF),
        ),
        in_specs=[smem()] + [vmem()] * 3,
        out_specs=(vmem(),) * 2,
        compiler_params=pltpu.CompilerParams(vmem_limit_bytes=4 * 1024 * 1024),
        cost_estimate=pl.CostEstimate(flops=1000000, bytes_accessed=1500000, transcendentals=0),
        name="assemble",
    )(pos, mine, near, far)


def conv_kernel_body(gated, halo, taps, scale, shift, out, ext):
    ext[0:32, :] = jnp.zeros((32, 256), F32)
    ext[544:560, :] = jnp.zeros((16, 256), F32)
    ext[2:32, :] = halo[...].astype(F32)
    ext[32:544, :] = gated[...].astype(F32)
    for lanes in (slice(0, 128), slice(128, 256)):
        for i in range(4):
            acc = jnp.zeros((128, 128), F32)
            for r in range(8):
                moved = ext[i * 128 + r : i * 128 + r + 160, lanes]
                for a in range(5):
                    j = a * 8 + r - 2
                    if 0 <= j < 31:
                        acc = acc + taps[j : j + 1, lanes] * moved[8 * a : 8 * a + 128]
            out[i, 0:128, lanes] = acc.astype(BF)
    extra = split3(scale[...]) + split3(shift[...]) + [jnp.zeros((10, 256), F32)]
    extra = jnp.concatenate(extra, axis=0).astype(BF)
    for i in range(4):
        out[i, 128:144, :] = extra


def convolve(gated, halo, taps, scale, shift):
    return pl.pallas_call(
        conv_kernel_body,
        out_shape=jax.ShapeDtypeStruct((4, 144, 256), BF),
        in_specs=[vmem()] * 5,
        out_specs=vmem(),
        scratch_shapes=[pltpu.VMEM((560, 256), F32)],
        compiler_params=pltpu.CompilerParams(vmem_limit_bytes=4 * 1024 * 1024),
        cost_estimate=pl.CostEstimate(flops=1000000000, bytes_accessed=800000, transcendentals=0),
        name="convolve",
    )(gated, halo, taps, scale, shift)


def split3(v):
    hi = v.astype(BF).astype(F32)
    mid = (v - hi).astype(BF).astype(F32)
    return [hi, mid, v - hi - mid]


def spans(pos):
    z, y, c = pos[0], pos[1], pos[2]

    def halves(z, y):
        return (z * 4 + y) * 2 + c, ((3 - z) * 4 + y) * 2 + 1 - c

    own = halves(z, y)
    over_y = [own] + [halves(z, lax.rem(y + d, 4)) for d in (3, 1, 2)]
    over_z = [own] + [halves(lax.rem(z + d, 4), y) for d in (3, 1, 2)]

    def pick(p, q):
        return [tuple(jnp.where(c == 0, u, v) for u, v in zip(m, n)) for m, n in zip(p, q)]

    return pick(over_y, over_z), pick(over_z, over_y)


def load_query(ref, qz, s):
    rows = lax.broadcasted_iota(jnp.int32, (128, 512), 0)
    for i in range(2):
        q = ref[:, i * 512 : (i + 1) * 512]
        qz[4 * s + 2 * i] = jnp.where(rows < 64, q, jnp.zeros_like(q))
        qz[4 * s + 2 * i + 1] = jnp.where(rows >= 64, q, jnp.zeros_like(q))


def load_keys(ref, kscr, vscr, b):
    for i in range(8):
        at = (i % 4) * 128
        kscr[2 * b + i // 4, at : at + 128, :] = ref[0:128, i * 128 : (i + 1) * 128]
    for j in range(2):
        vscr[2 * b + j] = ref[128:256, j * 512 : (j + 1) * 512]


def list_pairs(todo, pairs, queries, keys):
    n = jnp.int32(0)
    todo[0] = 0
    for s, b in pairs:
        for i in range(2):
            for j in range(2):
                ok = keys[b][j] < queries[s][i]
                code = s * 16 + i * 8 + b * 2 + j

                @pl.when(ok)
                def _(n=n, code=code):
                    todo[n] = code
                    todo[n + 1] = code

                n = n + ok.astype(jnp.int32)
    return n


def weigh(tacc, mref, r, cols, scores, masked):
    n, w = scores.shape
    s3 = scores.reshape(n // 8, 8, w)
    if mref is not None:
        s3 = s3 - mref[r, :, cols][None]
    p = jnp.exp2(s3).reshape(n, w)
    if masked:
        k = lax.broadcasted_iota(jnp.int32, (256, 256), 0)
        q = lax.broadcasted_iota(jnp.int32, (256, 256), 1)
        last = jnp.where(k <= q, p[n - 256 :], 0.0)
        p = last if n == 256 else jnp.concatenate([p[: n - 256], last], axis=0)
    tacc[r, :, cols] += jnp.sum(p.reshape(n // 8, 8, w), axis=0)
    return p.astype(BF)


def run_pairs(todo, n, qz, kscr, vscr, sbuf, pbuf, oacc, tacc, mref):
    def score(e, m):
        return jnp.dot(kscr[e & 7], qz[(e >> 3) * 2 + m], preferred_element_type=F32)

    @pl.when(n > 0)
    def _():
        sbuf[0] = score(todo[0], 0)

        @pl.loop(0, n)
        def _(t):
            e = todo[t]
            later = todo[t + 1]
            for m in range(2):
                sbuf[1 - m] = score(e, 1) if m == 0 else score(later, 0)
                r = (e >> 3) * 2 + m
                pbuf[m] = weigh(tacc, mref, r, slice(0, 512), sbuf[m], False)
                oacc[r] += jnp.dot(vscr[e & 7], pbuf[m], preferred_element_type=F32)


def run_diagonal(qz, kscr, vscr, sbuf, pbuf, oacc, tacc, mref):
    for h in range(2):
        for m in range(2):
            for qt in range(2):
                n = (qt + 1) * 256
                cols = slice(qt * 256, n)
                r = h * 2 + m
                sbuf[m, :n, cols] = jnp.dot(
                    kscr[h, :n, :], qz[r, :, cols], preferred_element_type=F32
                )
                pbuf[m, :n, cols] = weigh(tacc, mref, r, cols, sbuf[m, :n, cols], True)
                oacc[r, :, cols] += jnp.dot(
                    vscr[h, :, :n], pbuf[m, :n, cols], preferred_element_type=F32
                )


def take_tops(todo, n, sources, qz, kscr, tacc, mref):
    for s in sources:
        tacc[4 * s : 4 * s + 4] = jnp.full((4, 8, 512), -1e30, F32)

    def one(b, r, qt, masked):
        cols = pl.ds(pl.multiple_of(qt * 256, 256), 256)
        sc = jnp.dot(kscr[b], qz[r, :, cols], preferred_element_type=F32)
        if masked:
            k = lax.broadcasted_iota(jnp.int32, (512, 256), 0)
            q = lax.broadcasted_iota(jnp.int32, (512, 256), 1) + qt * 256
            sc = jnp.where(k <= q, sc, -1e30)
        tacc[r, :, cols] = jnp.maximum(tacc[r, :, cols], jnp.max(sc.reshape(64, 8, 256), axis=0))

    if 0 in sources:

        @pl.loop(0, 8)
        def _(i):
            one(i >> 2, i >> 1, i & 1, True)

    @pl.loop(0, n * 4)
    def _(i):
        e = todo[i >> 2]
        one(e & 7, (e >> 3) * 2 + ((i >> 1) & 1), i & 1, False)

    for s in sources:
        for r in range(4 * s, 4 * s + 4):
            mref[r] = jnp.broadcast_to(jnp.max(tacc[r], axis=0, keepdims=True), (8, 512))


def finish(sources, fast, pos, qz, kvs, kscr, vscr, sbuf, pbuf, oacc, tacc, mref, todo, flag):
    queries, keys = spans(pos)
    mref[...] = jnp.zeros_like(mref)
    flag[0] = 1

    @pl.loop(0, 2)
    def _(attempt):
        @pl.when(flag[0] == 1)
        def _():
            flag[1] = list_pairs(todo, fast, queries, keys)

            @pl.when(attempt == 1)
            def _():
                for b in range(4):
                    load_keys(kvs[b], kscr, vscr, b)
                every = [(s, b) for s in sources for b in range(4)]
                flag[1] = list_pairs(todo, every, queries, keys)
                take_tops(todo, flag[1], sources, qz, kscr, tacc, mref)
                for s in sources:
                    oacc[4 * s : 4 * s + 4] = jnp.zeros((4, 128, 512), F32)
                    tacc[4 * s : 4 * s + 4] = jnp.zeros((4, 8, 512), F32)
                if 0 in sources:
                    run_diagonal(qz, kscr, vscr, sbuf, pbuf, oacc, tacc, mref)

            run_pairs(todo, flag[1], qz, kscr, vscr, sbuf, pbuf, oacc, tacc, mref)
            worst = jnp.zeros((1, 512), F32)
            for s in sources:
                for i in range(2):
                    has = s == 0
                    for b in range(4):
                        for j in range(2):
                            has = jnp.logical_or(has, keys[b][j] < queries[s][i])
                    least = jnp.where(has, 1.0 / BIG, -1.0)
                    for m in range(2):
                        t = jnp.sum(tacc[4 * s + 2 * i + m], axis=0, keepdims=True)
                        good = jnp.logical_and(t < BIG, t > least)
                        worst = jnp.where(good, worst, 1.0)
            bad = (jnp.max(worst) > 0.5).astype(jnp.int32)
            flag[0] = jnp.where(attempt == 0, bad, 0)


def gathered(ref, s, m, axis):
    pieces = [ref[4 * s + 2 * i + m] for i in range(2)]
    if axis is not None:
        pieces = [jnp.sum(p, axis=0, keepdims=True) for p in pieces]
    return jnp.concatenate(pieces, axis=1)


def write_sum(ref, s, oacc, tacc, mref):
    extra = []
    for m in range(2):
        ref[m * 128 : (m + 1) * 128, :] = gathered(oacc, s, m, None).astype(BF)
        extra = extra + split3(gathered(tacc, s, m, 0))
    for m in range(2):
        extra = extra + split3(gathered(mref, s, m, None)[0:1])
    ref[256:272, :] = jnp.concatenate(extra + [jnp.zeros((4, 1024), F32)], axis=0).astype(BF)


def own_kernel(pos, q0, kv0, oacc, tacc, qz, kscr, vscr, sbuf, pbuf, todo):
    load_query(q0, qz, 0)
    load_keys(kv0, kscr, vscr, 0)
    oacc[...] = jnp.zeros_like(oacc)
    tacc[...] = jnp.zeros_like(tacc)
    run_diagonal(qz, kscr, vscr, sbuf, pbuf, oacc, tacc, None)


def near_kernel(
    pos, q0, q1, q2, kv0, kv1, kv2, oin, tin, oacc, tacc, qz, kscr, vscr, sbuf, pbuf, todo
):
    queries, keys = spans(pos)
    for s, ref in enumerate((q0, q1, q2)):
        load_query(ref, qz, s)
    for b, ref in enumerate((kv0, kv1, kv2)):
        load_keys(ref, kscr, vscr, b)
    n = list_pairs(todo, [(s, b) for b in range(3) for s in range(3)], queries, keys)
    run_pairs(todo, n, qz, kscr, vscr, sbuf, pbuf, oacc, tacc, None)


def mid_kernel(
    pos, q1, q2, kv0, kv1, kv2, kv3, oin, tin, oacc, tacc, out1, out2,
    qz, kscr, vscr, sbuf, pbuf, todo, mref, flag,
):
    for s, ref in enumerate((q1, q2)):
        load_query(ref, qz, s + 1)
    kvs = (kv0, kv1, kv2, kv3)
    load_keys(kv3, kscr, vscr, 3)
    fast = [(1, 3), (2, 3)]
    finish((1, 2), fast, pos, qz, kvs, kscr, vscr, sbuf, pbuf, oacc, tacc, mref, todo, flag)
    write_sum(out1, 1, oacc, tacc, mref)
    write_sum(out2, 2, oacc, tacc, mref)


def far_kernel(
    pos, q3, kv0, kv1, kv2, kv3, oin, tin, oacc, tacc, out3,
    qz, kscr, vscr, sbuf, pbuf, todo, mref, flag,
):
    load_query(q3, qz, 3)
    kvs = (kv0, kv1, kv2, kv3)
    for b in range(4):
        load_keys(kvs[b], kscr, vscr, b)
    fast = [(3, b) for b in range(4)]
    finish((3,), fast, pos, qz, kvs, kscr, vscr, sbuf, pbuf, oacc, tacc, mref, todo, flag)
    write_sum(out3, 3, oacc, tacc, mref)


def last_kernel(
    pos, q0, kv0, kv1, kv2, kv3, oin, tin, own, stats,
    qz, kscr, vscr, sbuf, pbuf, todo, mref, flag, tacc,
):
    own[...] = oin[0:4]
    tacc[...] = tin[0:4]
    load_query(q0, qz, 0)
    kvs = (kv0, kv1, kv2, kv3)
    load_keys(kv3, kscr, vscr, 3)
    finish((0,), [(0, 3)], pos, qz, kvs, kscr, vscr, sbuf, pbuf, own, tacc, mref, todo, flag)
    t = [gathered(tacc, 0, m, 0) for m in range(2)]
    top = [gathered(mref, 0, m, None)[0:1] for m in range(2)]
    stats[...] = jnp.concatenate(t + top + [jnp.zeros((4, 1024), F32)], axis=0)


def attention_call(body, ins, outs, pairs, carried=True, checked=True, sums=None, extra=()):
    sums = sums or (jax.ShapeDtypeStruct((16, 128, 512), F32), jax.ShapeDtypeStruct((16, 8, 512), F32))
    scratches = [
        pltpu.VMEM((16, 128, 512), BF),
        pltpu.VMEM((8, 512, 128), BF),
        pltpu.VMEM((8, 128, 512), BF),
        pltpu.VMEM((2, 512, 512), F32),
        pltpu.VMEM((2, 512, 512), BF),
        pltpu.SMEM((72,), jnp.int32),
    ]
    if checked:
        scratches += [pltpu.VMEM((16, 8, 512), F32), pltpu.SMEM((2,), jnp.int32), *extra]
    return pl.pallas_call(
        body,
        out_shape=(*sums, *outs),
        in_specs=[smem()] + [vmem()] * (len(ins) - 1),
        out_specs=(vmem(),) * (2 + len(outs)),
        scratch_shapes=scratches,
        input_output_aliases={len(ins) - 2: 0, len(ins) - 1: 1} if carried else {},
        compiler_params=pltpu.CompilerParams(vmem_limit_bytes=12 * 1024 * 1024),
        cost_estimate=pl.CostEstimate(
            flops=800000000 * pairs, bytes_accessed=4000000, transcendentals=2000000 * pairs
        ),
    )(*ins)


SENT = jax.ShapeDtypeStruct((272, 1024), BF)


def merge_kernel(pos, lam, own, stats, r1, r2, r3, gain, packed, lmine, lother):
    c = pos[2]
    mix = jnp.where(c == 0, lam[0], lam[1])

    def joined(ref, row):
        part = ref[256:272, :].astype(F32)
        return part[row : row + 1] + part[row + 1 : row + 2] + part[row + 2 : row + 3]

    heads = []
    logs = []
    for m in range(2):
        ts = [stats[m : m + 1, :]] + [joined(r, 3 * m) for r in (r1, r2, r3)]
        ms = [stats[2 + m : 3 + m, :]] + [joined(r, 6 + 3 * m) for r in (r1, r2, r3)]
        ms = [jnp.where(t > 0, v, -1e30) for t, v in zip(ts, ms)]
        top = jnp.maximum(jnp.maximum(ms[0], ms[1]), jnp.maximum(ms[2], ms[3]))
        ws = [jnp.exp2(v - top) for v in ms]
        total = ws[0] * ts[0] + ws[1] * ts[1] + ws[2] * ts[2] + ws[3] * ts[3]
        inv = 1.0 / total
        acc = jnp.concatenate([own[m], own[2 + m]], axis=1) * (ws[0] * inv)
        for w, r in zip(ws[1:], (r1, r2, r3)):
            acc = acc + r[m * 128 : (m + 1) * 128, :].astype(F32) * (w * inv)
        heads.append(acc)
        logs.append(top * math.log(2.0) + jnp.log(total))
    h = heads[0] - mix * heads[1]
    h = h * lax.rsqrt(jnp.mean(h * h, axis=0, keepdims=True) + 1e-06)
    lt = jnp.concatenate(logs, axis=0)
    for i in range(8):
        u = (i // 4) * 512 + (i % 4) * 128
        v = (1 - i // 4) * 512 + (i % 4) * 128
        part = jnp.where(c == 0, h[:, u : u + 128], h[:, v : v + 128])
        packed[i] = (part.T * gain[...]).astype(BF)
    lmine[...] = lt[:, :512]
    lother[...] = lt[:, 512:]


def merge(pos, lam, own, stats, parts, *rest):
    return pl.pallas_call(
        merge_kernel,
        out_shape=(
            jax.ShapeDtypeStruct((8, 128, 128), BF),
            jax.ShapeDtypeStruct((2, 512), F32),
            jax.ShapeDtypeStruct((2, 512), F32),
        ),
        in_specs=[smem(), smem()] + [vmem()] * 6,
        out_specs=(vmem(),) * 3,
        compiler_params=pltpu.CompilerParams(vmem_limit_bytes=8 * 1024 * 1024),
        cost_estimate=pl.CostEstimate(flops=500000000, bytes_accessed=4000000, transcendentals=0),
        name="merge",
    )(pos, lam, own, stats, *parts, *rest)


def fetches(w, first, held, sem):
    copies = [
        pltpu.make_async_copy(
            w.at[first : first + 1024, i * 512 : (i + 1) * 512], held.at[i], sem.at[i]
        )
        for i in range(4)
    ]
    for copy in copies:
        copy.start()
    return copies


def half_kernel(moved, token, w, out, lhs, held, sem):
    copies = fetches(w, 1024, held, sem)
    total = jnp.zeros((128, 1), F32)
    square = jnp.zeros((128, 1), F32)
    for k in range(4):
        v = moved[k, 0:128, :].astype(F32)
        total = total + jnp.sum(v, axis=1, keepdims=True)
        square = square + jnp.sum(v * v, axis=1, keepdims=True)
    middle = total * (1.0 / 1024)
    inv = lax.rsqrt(square * (1.0 / 1024) - middle * middle + 1e-05)
    for k in range(4):
        p = moved[k, 128:144, :].astype(F32)
        gain = p[0:1] + p[1:2] + p[2:3]
        shift = p[3:4] + p[4:5] + p[5:6]
        v = moved[k, 0:128, :].astype(F32)
        v = (v - middle) * inv * gain + shift
        lhs[:, k * 256 : (k + 1) * 256] = (v * jax.nn.sigmoid(v)).astype(BF)
    for i, copy in enumerate(copies):
        copy.wait()
        out[:, i * 512 : (i + 1) * 512] = jnp.dot(lhs[...], held[i], preferred_element_type=F32)


def output_kernel(moved, part, w, out, lhs, held, sem):
    copies = fetches(w, 0, held, sem)
    for c in range(2):
        for k in range(4):
            at = k * 256 + c * 128
            lhs[:, at : at + 128] = moved[c * 4 + k]
    for i, copy in enumerate(copies):
        copy.wait()
        cols = slice(i * 512, (i + 1) * 512)
        out[:, cols] = (
            part[:, cols] + jnp.dot(lhs[...], held[i], preferred_element_type=F32)
        ).astype(BF)


def product(body, dtype, moved, other, w):
    return pl.pallas_call(
        body,
        out_shape=jax.ShapeDtypeStruct((128, 2048), dtype),
        in_specs=[vmem(), vmem(), hbm()],
        out_specs=vmem(),
        scratch_shapes=[
            pltpu.VMEM((128, 1024), BF),
            pltpu.VMEM((4, 1024, 512), BF),
            pltpu.SemaphoreType.DMA((4,)),
        ],
        compiler_params=pltpu.CompilerParams(vmem_limit_bytes=52 * 1024 * 1024),
        cost_estimate=pl.CostEstimate(flops=600000000, bytes_accessed=5000000, transcendentals=0),
    )(moved, other, w)


def per_device_steps(
    tokens, norm_gain, query_weight, key_weight, value_weight, glu_value_weight, glu_gate_weight,
    qk_gain, mix_lambda, head_gain, conv_kernel, channel_gain, channel_shift, output_weight,
):
    sp = lax.axis_index("sp").astype(jnp.int32)
    tp = lax.axis_index("tp").astype(jnp.int32)
    core = sp % NC
    pos = jnp.stack([sp // (NY * NC), (sp // NC) % NY, core, tp])
    upper, lower = tokens[:64], tokens[64:]
    a1 = along_x(upper, 1)
    a2 = along_x(lower, -1)
    b1 = along_x(lower, 1)
    b2 = along_x(upper, -1)
    f1 = along_x(a1, 1)
    f2 = along_x(a2, -1)
    place = (sp * 512 + jnp.arange(512, dtype=jnp.int32)).astype(F32)
    inverse = 10000.0 ** (-jnp.arange(0, 32, dtype=F32) * 2.0 / 64)
    angles = place[:, None] * inverse[None, :]
    cosine = jnp.cos(angles)
    sine = jnp.sin(angles)
    cos = jnp.concatenate([cosine] * 4, axis=1)
    sin = jnp.concatenate([-sine, sine, -sine, sine], axis=1)
    qkg = jnp.tile(qk_gain.reshape(1, 128), (1, 2))
    t0, *weights = prefetch(
        (tokens, query_weight, key_weight, value_weight, glu_value_weight, glu_gate_weight),
        cos,
        sin,
    )
    shared = (
        norm_gain[None, :],
        *weights,
        qkg,
        cos,
        sin,
    )
    mine, gated, given = project(project_first, 384, pos, (t0, a1, b1, b2, a2), shared, ())
    near_in = to_mirror(given)
    mine, gated, given = project(project_last, 128, pos, (f1, f2), shared, (mine, gated))
    far_in = to_mirror(given)
    halo = lax.ppermute(
        gated[482:], "sp", [(i, i + 1) for i in range(NZ * NY * NC - 1)]
    )
    q, kv = assemble(pos, mine, near_in, far_in)
    kv1 = send_keys(kv, 1)
    kv2 = send_keys(kv, -1)
    q1 = send_query(q, 1)
    q2 = send_query(q, -1)
    q3 = send_query(q, 2)
    kv3 = send_keys(kv, 2)
    sums = attention_call(own_kernel, (pos, q, kv), (), 1, carried=False, checked=False)
    sums = attention_call(near_kernel, (pos, q, q1, q2, kv, kv1, kv2, *sums), (), 8, checked=False)
    *sums, o1, o2 = attention_call(
        mid_kernel, (pos, q1, q2, kv, kv1, kv2, kv3, *sums), (SENT,) * 2, 2
    )
    r1 = send_query(o1, -1)
    r2 = send_query(o2, 1)
    *sums, o3 = attention_call(far_kernel, (pos, q3, kv, kv1, kv2, kv3, *sums), (SENT,), 4)
    r3 = send_query(o3, 2)
    own, stats = attention_call(
        last_kernel,
        (pos, q, kv, kv1, kv2, kv3, *sums),
        (),
        1,
        carried=False,
        sums=(
            jax.ShapeDtypeStruct((4, 128, 512), F32),
            jax.ShapeDtypeStruct((8, 1024), F32),
        ),
        extra=(pltpu.VMEM((4, 8, 512), F32),),
    )
    conv = convolve(gated, halo, conv_kernel, channel_gain[None, :], channel_shift[None, :])
    conv, stats = lax.optimization_barrier((conv, stats))
    conv = lax.all_to_all(conv, "tp", split_axis=0, concat_axis=0, tiled=True)
    packed, lmine, lother = merge(
        pos,
        mix_lambda,
        own,
        stats,
        (r1, r2, r3),
        head_gain[None, :],
    )
    groups = []
    for z in range(NZ):
        for y in range(NY):
            ends = ((z * NY + y) * NC, ((NZ - 1 - z) * NY + y) * NC + 1)
            groups.append([end * 4 + x for end in ends for x in range(4)])
    moved = lax.all_to_all(
        packed, ("sp", "tp"), split_axis=0, concat_axis=0, axis_index_groups=groups, tiled=True
    )
    ltheirs = to_mirror(lother)
    log_totals = jnp.where(
        core == 0, jnp.stack([lmine, ltheirs], axis=1), jnp.stack([ltheirs, lmine], axis=1)
    )
    part = product(half_kernel, F32, conv, lmine, output_weight)
    mixed = product(output_kernel, BF, moved, part, output_weight)
    return (mixed, log_totals)


def solution(mesh):
    placed = (
        P(("sp", "tp"), None),
        P(),
        P(None, "tp"),
        P(None, "tp"),
        P(None, "tp"),
        P(None, "tp"),
        P(None, "tp"),
        P(),
        P("tp"),
        P(),
        P(None, "tp"),
        P("tp"),
        P("tp"),
        P(),
    )
    return jax.shard_map(
        per_device_steps,
        mesh=mesh,
        in_specs=placed,
        out_specs=(P(("sp", "tp"), None), P(None, "tp", "sp")),
        check_vma=False,
    )
```

```python
import math

import jax
import jax.numpy as jnp
from jax import lax
from jax.experimental import pallas as pl
from jax.experimental.pallas import tpu as pltpu
from jax.sharding import PartitionSpec as P

NZ, NY, NC = 4, 4, 2
BIG = 2.0**100
LOG2E = math.log2(math.e)
BF = jnp.bfloat16
F32 = jnp.float32


def vmem():
    return pl.BlockSpec(memory_space=pltpu.VMEM)


def smem():
    return pl.BlockSpec(memory_space=pltpu.SMEM)


def moves(target):
    out = []
    for z in range(NZ):
        for y in range(NY):
            for c in range(NC):
                t = target(z, y, c)
                if t is not None:
                    out.append(((z * NY + y) * NC + c, (t[0] * NY + t[1]) * NC + t[2]))
    return out


def stepped(z, y, along_y, step):
    return (z, (y + step) % NY) if along_y else ((z + step) % NZ, y)


def send_query(value, step):
    return lax.ppermute(
        value, "sp", moves(lambda z, y, c: (*stepped(z, y, c == 0, step), c))
    )


def send_keys(value, step):
    return lax.ppermute(
        value, "sp", moves(lambda z, y, c: (*stepped(z, y, c == 1, step), c))
    )


def to_mirror(value):
    return lax.ppermute(value, "sp", moves(lambda z, y, c: (NZ - 1 - z, y, 1 - c)))


def along_x(value, step):
    count = lax.axis_size("tp")
    return lax.ppermute(value, "tp", [(i, (i + step) % count) for i in range(count)])


def hbm():
    return pl.BlockSpec(memory_space=pl.ANY)


def prefetch_kernel(*refs):
    n = (len(refs) - 3) // 2
    copies = [
        pltpu.make_async_copy(refs[i], refs[n + 2 + i], refs[2 * n + 2].at[i]) for i in range(n)
    ]
    for copy in copies:
        copy.start()
    for copy in copies:
        copy.wait()


def prefetch(arrays, *tables):
    return pl.pallas_call(
        prefetch_kernel,
        out_shape=tuple(jax.ShapeDtypeStruct(a.shape, a.dtype) for a in arrays),
        in_specs=[hbm()] * len(arrays) + [vmem()] * 2,
        out_specs=(vmem(),) * len(arrays),
        scratch_shapes=[pltpu.SemaphoreType.DMA((len(arrays),))],
        compiler_params=pltpu.CompilerParams(vmem_limit_bytes=48 * 1024 * 1024),
        cost_estimate=pl.CostEstimate(flops=2000000, bytes_accessed=12000000, transcendentals=0),
        name="prefetch",
    )(*arrays, *tables)


def project_body(pos, pieces, gain, ws, qkg, cos, sin, mine, other, gated, normed):
    x = pos[3]
    c = pos[2]
    ats = []
    row = 0
    for ref, step in pieces:
        t = ref[...].astype(F32)
        n = t.shape[0]
        ms = jnp.mean(t * t, axis=-1, keepdims=True)
        normed[row : row + n, :] = (t * lax.rsqrt(ms + 1e-06) * gain[...]).astype(BF)
        if row % 128 == 0:
            ats.append(pl.multiple_of(lax.rem(x + step, 4) * 128, 128))
        row += n
    lane = lax.broadcasted_iota(jnp.int32, (1, 256), 1)
    first = lax.rem(lane, 64) < 32
    gi = lax.broadcasted_iota(jnp.int32, (256, 256), 0) // 64
    gj = lax.broadcasted_iota(jnp.int32, (256, 256), 1) // 64
    groups = jnp.where(gi == gj, 1.0 / 64, 0.0).astype(BF)

    spread = lax.broadcasted_iota(jnp.int32, (64, 256), 0)
    spread = (spread == lax.rem(lax.broadcasted_iota(jnp.int32, (64, 256), 1), 64)).astype(BF)
    rows = [
        jnp.dot(part.astype(BF), spread, preferred_element_type=F32) for part in split3(qkg[...])
    ]
    rows = rows[0] + rows[1] + rows[2]
    gains = jnp.where(lax.rem(lane // 64, 2) == 0, rows[0:1], rows[1:2])

    def table(ref):
        v = jnp.concatenate([ref[pl.ds(at, 128), :] for at in ats], axis=0)
        return jnp.concatenate([v, v], axis=1)

    cc = table(cos)
    ss = table(sin)

    def times(w):
        return jnp.dot(normed[...], w[...], preferred_element_type=F32).astype(BF).astype(F32)

    def turned(w):
        v = times(w)
        sq = v * v
        hi = sq.astype(BF)
        lo = (sq - hi.astype(F32)).astype(BF)
        ms = jnp.dot(hi, groups, preferred_element_type=F32) + jnp.dot(
            lo, groups, preferred_element_type=F32
        )
        v = v * lax.rsqrt(ms + 1e-06) * gains
        swapped = jnp.where(first, pltpu.roll(v, 256 - 32, 1), pltpu.roll(v, 32, 1))
        return v * cc + swapped * ss

    def put(row, v, flip):
        a = v[:, :128]
        b = v[:, 128:]
        kept = jnp.where(c == 0, a, b)
        given = jnp.where(c == 0, b, a)
        for i, at in enumerate(ats):
            rows = slice(i * 128, (i + 1) * 128)
            part = kept[rows, :]
            mine[row : row + 128, pl.ds(at, 128)] = (part.T if flip else part).astype(BF)
            part = given[rows, :]
            other[row : row + 128, rows] = (part.T if flip else part).astype(BF)

    wq, wk, wv, wa, wg = ws
    put(0, turned(wq) * 0.125, True)
    put(128, turned(wk), False)
    put(256, times(wv), True)
    g = times(wa) * jax.nn.sigmoid(times(wg))
    for i, at in enumerate(ats):
        gated[pl.ds(at, 128), :] = g[i * 128 : (i + 1) * 128, :].astype(BF)


def project_first(
    pos, t0, t1, a1, b1, b2, a2, gain, wq, wk, wv, wa, wg, qkg, cos, sin, mine, gated, other, normed
):
    project_body(
        pos, ((t0, 0), (t1, 0), (a1, 3), (b1, 3), (b2, 1), (a2, 1)), gain, (wq, wk, wv, wa, wg), qkg, cos,
        sin, mine, other, gated, normed,
    )


def project_last(
    pos, f1, f2, gain, wq, wk, wv, wa, wg, qkg, cos, sin, mine_in, gated_in, mine, gated, other,
    normed,
):
    project_body(
        pos, ((f1, 2), (f2, 2)), gain, (wq, wk, wv, wa, wg), qkg, cos, sin,
        mine, other, gated, normed,
    )


def project(body, rows, pos, pieces, shared, filled):
    count = 1 + len(pieces) + len(shared) + len(filled)
    start = count - len(filled)
    return pl.pallas_call(
        body,
        out_shape=(
            jax.ShapeDtypeStruct((384, 512), BF),
            jax.ShapeDtypeStruct((512, 256), BF),
            jax.ShapeDtypeStruct((384, rows), BF),
        ),
        in_specs=[smem()] + [vmem()] * (count - 1),
        out_specs=(vmem(),) * 3,
        scratch_shapes=[pltpu.VMEM((rows, 2048), BF)],
        input_output_aliases={start + i: i for i in range(len(filled))},
        compiler_params=pltpu.CompilerParams(vmem_limit_bytes=14 * 1024 * 1024),
        cost_estimate=pl.CostEstimate(
            flops=5242880 * rows, bytes_accessed=8000000, transcendentals=0
        ),
    )(pos, *pieces, *shared, *filled)


def assemble_kernel(pos, mine, near, far, q, kv):
    x = pos[3]
    q[:, 0:512] = mine[0:128, :]
    kv[:, 0:512] = mine[128:384, :]
    for i, step in enumerate((0, 3, 1, 2)):
        at = pl.multiple_of(512 + lax.rem(x + step, 4) * 128, 128)
        ref = near if i < 3 else far
        cols = slice(i * 128, (i + 1) * 128) if i < 3 else slice(0, 128)
        q[:, pl.ds(at, 128)] = ref[0:128, cols]
        kv[:, pl.ds(at, 128)] = ref[128:384, cols]


def assemble(pos, mine, near, far):
    return pl.pallas_call(
        assemble_kernel,
        out_shape=(
            jax.ShapeDtypeStruct((128, 1024), BF),
            jax.ShapeDtypeStruct((256, 1024), BF),
        ),
        in_specs=[smem()] + [vmem()] * 3,
        out_specs=(vmem(),) * 2,
        compiler_params=pltpu.CompilerParams(vmem_limit_bytes=4 * 1024 * 1024),
        cost_estimate=pl.CostEstimate(flops=1000000, bytes_accessed=1500000, transcendentals=0),
        name="assemble",
    )(pos, mine, near, far)


def conv_kernel_body(gated, halo, taps, scale, shift, out, ext):
    for h in range(2):
        lanes = slice(h * 128, (h + 1) * 128)
        ext[h, 0:32, :] = jnp.zeros((32, 128), F32)
        ext[h, 544:560, :] = jnp.zeros((16, 128), F32)
        ext[h, 2:32, :] = halo[:, lanes].astype(F32)
        ext[h, 32:544, :] = gated[:, lanes].astype(F32)
        for i in range(4):
            acc = jnp.zeros((128, 128), F32)
            for r in range(8):
                moved = ext[h, i * 128 + r : i * 128 + r + 160, :]
                for a in range(5):
                    j = a * 8 + r - 2
                    if 0 <= j < 31:
                        acc = acc + taps[j : j + 1, lanes] * moved[8 * a : 8 * a + 128]
            out[i, 0:128, lanes] = acc.astype(BF)
    extra = split3(scale[...]) + split3(shift[...]) + [jnp.zeros((10, 256), F32)]
    extra = jnp.concatenate(extra, axis=0).astype(BF)
    for i in range(4):
        out[i, 128:144, :] = extra


def convolve(gated, halo, taps, scale, shift):
    return pl.pallas_call(
        conv_kernel_body,
        out_shape=jax.ShapeDtypeStruct((4, 144, 256), BF),
        in_specs=[vmem()] * 5,
        out_specs=vmem(),
        scratch_shapes=[pltpu.VMEM((2, 560, 128), F32)],
        compiler_params=pltpu.CompilerParams(vmem_limit_bytes=4 * 1024 * 1024),
        cost_estimate=pl.CostEstimate(flops=1000000000, bytes_accessed=800000, transcendentals=0),
        name="convolve",
    )(gated, halo, taps, scale, shift)


def split3(v):
    hi = v.astype(BF).astype(F32)
    mid = (v - hi).astype(BF).astype(F32)
    return [hi, mid, v - hi - mid]


def spans(pos):
    z, y, c = pos[0], pos[1], pos[2]

    def halves(z, y):
        return (z * 4 + y) * 2 + c, ((3 - z) * 4 + y) * 2 + 1 - c

    own = halves(z, y)
    over_y = [own] + [halves(z, lax.rem(y + d, 4)) for d in (3, 1, 2)]
    over_z = [own] + [halves(lax.rem(z + d, 4), y) for d in (3, 1, 2)]

    def pick(p, q):
        return [tuple(jnp.where(c == 0, u, v) for u, v in zip(m, n)) for m, n in zip(p, q)]

    return pick(over_y, over_z), pick(over_z, over_y)


def load_query(ref, qz, s):
    rows = lax.broadcasted_iota(jnp.int32, (128, 512), 0)
    for i in range(2):
        q = ref[:, i * 512 : (i + 1) * 512]
        qz[4 * s + 2 * i] = jnp.where(rows < 64, q, jnp.zeros_like(q))
        qz[4 * s + 2 * i + 1] = jnp.where(rows >= 64, q, jnp.zeros_like(q))


def load_keys(ref, kscr, vscr, b):
    for i in range(8):
        at = (i % 4) * 128
        kscr[2 * b + i // 4, at : at + 128, :] = ref[0:128, i * 128 : (i + 1) * 128]
    for j in range(2):
        vscr[2 * b + j] = ref[128:256, j * 512 : (j + 1) * 512]


def list_pairs(todo, pairs, queries, keys):
    n = jnp.int32(0)
    todo[0] = 0
    for s, b in pairs:
        for i in range(2):
            for j in range(2):
                ok = keys[b][j] < queries[s][i]
                code = s * 16 + i * 8 + b * 2 + j

                @pl.when(ok)
                def _(n=n, code=code):
                    todo[n] = code
                    todo[n + 1] = code

                n = n + ok.astype(jnp.int32)
    return n


def weigh(tacc, mref, r, cols, scores, masked):
    n, w = scores.shape
    s3 = scores.reshape(n // 8, 8, w) * LOG2E
    if mref is not None:
        s3 = s3 - mref[r, :, cols][None]
    p = jnp.exp2(s3).reshape(n, w)
    if masked:
        k = lax.broadcasted_iota(jnp.int32, (256, 256), 0)
        q = lax.broadcasted_iota(jnp.int32, (256, 256), 1)
        last = jnp.where(k <= q, p[n - 256 :], 0.0)
        p = last if n == 256 else jnp.concatenate([p[: n - 256], last], axis=0)
    tacc[r, :, cols] += jnp.sum(p.reshape(n // 8, 8, w), axis=0)
    return p.astype(BF)


def run_pairs(todo, n, qz, kscr, vscr, sbuf, pbuf, oacc, tacc, mref):
    def score(e, m):
        return jnp.dot(kscr[e & 7], qz[(e >> 3) * 2 + m], preferred_element_type=F32)

    @pl.when(n > 0)
    def _():
        sbuf[0] = score(todo[0], 0)

        @pl.loop(0, n)
        def _(t):
            e = todo[t]
            later = todo[t + 1]
            for m in range(2):
                sbuf[1 - m] = score(e, 1) if m == 0 else score(later, 0)
                r = (e >> 3) * 2 + m
                pbuf[m] = weigh(tacc, mref, r, slice(0, 512), sbuf[m], False)
                oacc[r] += jnp.dot(vscr[e & 7], pbuf[m], preferred_element_type=F32)


def run_diagonal(qz, kscr, vscr, sbuf, pbuf, oacc, tacc, mref):
    for h in range(2):
        for m in range(2):
            for qt in range(2):
                n = (qt + 1) * 256
                cols = slice(qt * 256, n)
                r = h * 2 + m
                sbuf[m, :n, cols] = jnp.dot(
                    kscr[h, :n, :], qz[r, :, cols], preferred_element_type=F32
                )
                pbuf[m, :n, cols] = weigh(tacc, mref, r, cols, sbuf[m, :n, cols], True)
                oacc[r, :, cols] += jnp.dot(
                    vscr[h, :, :n], pbuf[m, :n, cols], preferred_element_type=F32
                )


def take_tops(todo, n, sources, qz, kscr, tacc, mref):
    for s in sources:
        tacc[4 * s : 4 * s + 4] = jnp.full((4, 8, 512), -1e30, F32)

    def one(b, r, qt, masked):
        cols = pl.ds(pl.multiple_of(qt * 256, 256), 256)
        sc = jnp.dot(kscr[b], qz[r, :, cols], preferred_element_type=F32)
        if masked:
            k = lax.broadcasted_iota(jnp.int32, (512, 256), 0)
            q = lax.broadcasted_iota(jnp.int32, (512, 256), 1) + qt * 256
            sc = jnp.where(k <= q, sc, -1e30)
        tacc[r, :, cols] = jnp.maximum(tacc[r, :, cols], jnp.max(sc.reshape(64, 8, 256), axis=0))

    if 0 in sources:

        @pl.loop(0, 8)
        def _(i):
            one(i >> 2, i >> 1, i & 1, True)

    @pl.loop(0, n * 4)
    def _(i):
        e = todo[i >> 2]
        one(e & 7, (e >> 3) * 2 + ((i >> 1) & 1), i & 1, False)

    for s in sources:
        for r in range(4 * s, 4 * s + 4):
            top = jnp.max(tacc[r], axis=0, keepdims=True) * LOG2E
            mref[r] = jnp.broadcast_to(top, (8, 512))


def finish(sources, fast, pos, qz, kvs, kscr, vscr, sbuf, pbuf, oacc, tacc, mref, todo, flag):
    queries, keys = spans(pos)
    mref[...] = jnp.zeros_like(mref)
    flag[0] = 1

    @pl.loop(0, 2)
    def _(attempt):
        @pl.when(flag[0] == 1)
        def _():
            flag[1] = list_pairs(todo, fast, queries, keys)

            @pl.when(attempt == 1)
            def _():
                for b in range(4):
                    load_keys(kvs[b], kscr, vscr, b)
                every = [(s, b) for s in sources for b in range(4)]
                flag[1] = list_pairs(todo, every, queries, keys)
                take_tops(todo, flag[1], sources, qz, kscr, tacc, mref)
                for s in sources:
                    oacc[4 * s : 4 * s + 4] = jnp.zeros((4, 128, 512), F32)
                    tacc[4 * s : 4 * s + 4] = jnp.zeros((4, 8, 512), F32)
                if 0 in sources:
                    run_diagonal(qz, kscr, vscr, sbuf, pbuf, oacc, tacc, mref)

            run_pairs(todo, flag[1], qz, kscr, vscr, sbuf, pbuf, oacc, tacc, mref)
            worst = jnp.zeros((1, 512), F32)
            for s in sources:
                for i in range(2):
                    has = s == 0
                    for b in range(4):
                        for j in range(2):
                            has = jnp.logical_or(has, keys[b][j] < queries[s][i])
                    least = jnp.where(has, 1.0 / BIG, -1.0)
                    for m in range(2):
                        t = jnp.sum(tacc[4 * s + 2 * i + m], axis=0, keepdims=True)
                        good = jnp.logical_and(t < BIG, t > least)
                        worst = jnp.where(good, worst, 1.0)
            bad = (jnp.max(worst) > 0.5).astype(jnp.int32)
            flag[0] = jnp.where(attempt == 0, bad, 0)


def gathered(ref, s, m, axis):
    pieces = [ref[4 * s + 2 * i + m] for i in range(2)]
    if axis is not None:
        pieces = [jnp.sum(p, axis=0, keepdims=True) for p in pieces]
    return jnp.concatenate(pieces, axis=1)


def write_sum(ref, s, oacc, tacc, mref):
    extra = []
    for m in range(2):
        ref[m * 128 : (m + 1) * 128, :] = gathered(oacc, s, m, None).astype(BF)
        extra = extra + split3(gathered(tacc, s, m, 0))
    for m in range(2):
        extra = extra + split3(gathered(mref, s, m, None)[0:1])
    ref[256:272, :] = jnp.concatenate(extra + [jnp.zeros((4, 1024), F32)], axis=0).astype(BF)


def own_kernel(pos, q0, kv0, oacc, tacc, qz, kscr, vscr, sbuf, pbuf, todo):
    load_query(q0, qz, 0)
    load_keys(kv0, kscr, vscr, 0)
    oacc[...] = jnp.zeros_like(oacc)
    tacc[...] = jnp.zeros_like(tacc)
    run_diagonal(qz, kscr, vscr, sbuf, pbuf, oacc, tacc, None)


def near_kernel(
    pos, q0, q1, q2, kv0, kv1, kv2, oin, tin, oacc, tacc, qz, kscr, vscr, sbuf, pbuf, todo
):
    queries, keys = spans(pos)
    for s, ref in enumerate((q0, q1, q2)):
        load_query(ref, qz, s)
    for b, ref in enumerate((kv0, kv1, kv2)):
        load_keys(ref, kscr, vscr, b)
    n = list_pairs(todo, [(s, b) for b in range(3) for s in range(3)], queries, keys)
    run_pairs(todo, n, qz, kscr, vscr, sbuf, pbuf, oacc, tacc, None)


def mid_kernel(
    pos, q1, q2, kv0, kv1, kv2, kv3, oin, tin, oacc, tacc, out1, out2,
    qz, kscr, vscr, sbuf, pbuf, todo, mref, flag,
):
    for s, ref in enumerate((q1, q2)):
        load_query(ref, qz, s + 1)
    kvs = (kv0, kv1, kv2, kv3)
    load_keys(kv3, kscr, vscr, 3)
    fast = [(1, 3), (2, 3)]
    finish((1, 2), fast, pos, qz, kvs, kscr, vscr, sbuf, pbuf, oacc, tacc, mref, todo, flag)
    write_sum(out1, 1, oacc, tacc, mref)
    write_sum(out2, 2, oacc, tacc, mref)


def far_kernel(
    pos, q3, kv0, kv1, kv2, kv3, oin, tin, oacc, tacc, out3,
    qz, kscr, vscr, sbuf, pbuf, todo, mref, flag,
):
    load_query(q3, qz, 3)
    kvs = (kv0, kv1, kv2, kv3)
    for b in range(4):
        load_keys(kvs[b], kscr, vscr, b)
    fast = [(3, b) for b in range(4)]
    finish((3,), fast, pos, qz, kvs, kscr, vscr, sbuf, pbuf, oacc, tacc, mref, todo, flag)
    write_sum(out3, 3, oacc, tacc, mref)


def last_kernel(
    pos, q0, kv0, kv1, kv2, kv3, oin, tin, own, stats,
    qz, kscr, vscr, sbuf, pbuf, todo, mref, flag, tacc,
):
    own[...] = oin[0:4]
    tacc[...] = tin[0:4]
    load_query(q0, qz, 0)
    kvs = (kv0, kv1, kv2, kv3)
    load_keys(kv3, kscr, vscr, 3)
    finish((0,), [(0, 3)], pos, qz, kvs, kscr, vscr, sbuf, pbuf, own, tacc, mref, todo, flag)
    t = [gathered(tacc, 0, m, 0) for m in range(2)]
    top = [gathered(mref, 0, m, None)[0:1] for m in range(2)]
    stats[...] = jnp.concatenate(t + top + [jnp.zeros((4, 1024), F32)], axis=0)


def attention_call(body, ins, outs, pairs, carried=True, checked=True, sums=None, extra=()):
    sums = sums or (jax.ShapeDtypeStruct((16, 128, 512), F32), jax.ShapeDtypeStruct((16, 8, 512), F32))
    scratches = [
        pltpu.VMEM((16, 128, 512), BF),
        pltpu.VMEM((8, 512, 128), BF),
        pltpu.VMEM((8, 128, 512), BF),
        pltpu.VMEM((2, 512, 512), F32),
        pltpu.VMEM((2, 512, 512), BF),
        pltpu.SMEM((72,), jnp.int32),
    ]
    if checked:
        scratches += [pltpu.VMEM((16, 8, 512), F32), pltpu.SMEM((2,), jnp.int32), *extra]
    return pl.pallas_call(
        body,
        out_shape=(*sums, *outs),
        in_specs=[smem()] + [vmem()] * (len(ins) - 1),
        out_specs=(vmem(),) * (2 + len(outs)),
        scratch_shapes=scratches,
        input_output_aliases={len(ins) - 2: 0, len(ins) - 1: 1} if carried else {},
        compiler_params=pltpu.CompilerParams(vmem_limit_bytes=12 * 1024 * 1024),
        cost_estimate=pl.CostEstimate(
            flops=800000000 * pairs, bytes_accessed=4000000, transcendentals=2000000 * pairs
        ),
    )(*ins)


SENT = jax.ShapeDtypeStruct((272, 1024), BF)


def merge_kernel(pos, lam, own, stats, r1, r2, r3, gain, packed, lmine, lother):
    c = pos[2]
    mix = jnp.where(c == 0, lam[0], lam[1])

    def joined(ref, row):
        part = ref[256:272, :].astype(F32)
        return part[row : row + 1] + part[row + 1 : row + 2] + part[row + 2 : row + 3]

    heads = []
    logs = []
    for m in range(2):
        ts = [stats[m : m + 1, :]] + [joined(r, 3 * m) for r in (r1, r2, r3)]
        ms = [stats[2 + m : 3 + m, :]] + [joined(r, 6 + 3 * m) for r in (r1, r2, r3)]
        ms = [jnp.where(t > 0, v, -1e30) for t, v in zip(ts, ms)]
        top = jnp.maximum(jnp.maximum(ms[0], ms[1]), jnp.maximum(ms[2], ms[3]))
        ws = [jnp.exp2(v - top) for v in ms]
        total = ws[0] * ts[0] + ws[1] * ts[1] + ws[2] * ts[2] + ws[3] * ts[3]
        inv = 1.0 / total
        acc = jnp.concatenate([own[m], own[2 + m]], axis=1) * (ws[0] * inv)
        for w, r in zip(ws[1:], (r1, r2, r3)):
            acc = acc + r[m * 128 : (m + 1) * 128, :].astype(F32) * (w * inv)
        heads.append(acc)
        logs.append(top * math.log(2.0) + jnp.log(total))
    h = heads[0] - mix * heads[1]
    h = h * lax.rsqrt(jnp.mean(h * h, axis=0, keepdims=True) + 1e-06)
    lt = jnp.concatenate(logs, axis=0)
    for i in range(8):
        u = (i // 4) * 512 + (i % 4) * 128
        v = (1 - i // 4) * 512 + (i % 4) * 128
        part = jnp.where(c == 0, h[:, u : u + 128], h[:, v : v + 128])
        packed[i] = (part.T * gain[...]).astype(BF)
    lmine[...] = lt[:, :512]
    lother[...] = lt[:, 512:]


def merge(pos, lam, own, stats, parts, *rest):
    return pl.pallas_call(
        merge_kernel,
        out_shape=(
            jax.ShapeDtypeStruct((8, 128, 128), BF),
            jax.ShapeDtypeStruct((2, 512), F32),
            jax.ShapeDtypeStruct((2, 512), F32),
        ),
        in_specs=[smem(), smem()] + [vmem()] * 6,
        out_specs=(vmem(),) * 3,
        compiler_params=pltpu.CompilerParams(vmem_limit_bytes=8 * 1024 * 1024),
        cost_estimate=pl.CostEstimate(flops=500000000, bytes_accessed=4000000, transcendentals=0),
        name="merge",
    )(pos, lam, own, stats, *parts, *rest)


def fetches(w, first, held, sem):
    copies = [
        pltpu.make_async_copy(
            w.at[first : first + 1024, i * 512 : (i + 1) * 512], held.at[i], sem.at[i]
        )
        for i in range(4)
    ]
    for copy in copies:
        copy.start()
    return copies


def half_kernel(moved, token, w, out, lhs, held, sem):
    copies = fetches(w, 1024, held, sem)
    total = jnp.zeros((128, 1), F32)
    square = jnp.zeros((128, 1), F32)
    for k in range(4):
        v = moved[k, 0:128, :].astype(F32)
        total = total + jnp.sum(v, axis=1, keepdims=True)
        square = square + jnp.sum(v * v, axis=1, keepdims=True)
    middle = total * (1.0 / 1024)
    inv = lax.rsqrt(square * (1.0 / 1024) - middle * middle + 1e-05)
    for k in range(4):
        p = moved[k, 128:144, :].astype(F32)
        gain = p[0:1] + p[1:2] + p[2:3]
        shift = p[3:4] + p[4:5] + p[5:6]
        v = moved[k, 0:128, :].astype(F32)
        v = (v - middle) * inv * gain + shift
        lhs[:, k * 256 : (k + 1) * 256] = (v * jax.nn.sigmoid(v)).astype(BF)
    for i, copy in enumerate(copies):
        copy.wait()
        out[:, i * 512 : (i + 1) * 512] = jnp.dot(lhs[...], held[i], preferred_element_type=F32)


def output_kernel(moved, part, w, out, lhs, held, sem):
    copies = fetches(w, 0, held, sem)
    for c in range(2):
        for k in range(4):
            at = k * 256 + c * 128
            lhs[:, at : at + 128] = moved[c * 4 + k]
    for i, copy in enumerate(copies):
        copy.wait()
        cols = slice(i * 512, (i + 1) * 512)
        out[:, cols] = (
            part[:, cols] + jnp.dot(lhs[...], held[i], preferred_element_type=F32)
        ).astype(BF)


def product(body, dtype, moved, other, w):
    return pl.pallas_call(
        body,
        out_shape=jax.ShapeDtypeStruct((128, 2048), dtype),
        in_specs=[vmem(), vmem(), hbm()],
        out_specs=vmem(),
        scratch_shapes=[
            pltpu.VMEM((128, 1024), BF),
            pltpu.VMEM((4, 1024, 512), BF),
            pltpu.SemaphoreType.DMA((4,)),
        ],
        compiler_params=pltpu.CompilerParams(vmem_limit_bytes=52 * 1024 * 1024),
        cost_estimate=pl.CostEstimate(flops=600000000, bytes_accessed=5000000, transcendentals=0),
    )(moved, other, w)


def per_device_steps(
    tokens, norm_gain, query_weight, key_weight, value_weight, glu_value_weight, glu_gate_weight,
    qk_gain, mix_lambda, head_gain, conv_kernel, channel_gain, channel_shift, output_weight,
):
    sp = lax.axis_index("sp").astype(jnp.int32)
    tp = lax.axis_index("tp").astype(jnp.int32)
    core = sp % NC
    pos = jnp.stack([sp // (NY * NC), (sp // NC) % NY, core, tp])
    upper, lower = tokens[:64], tokens[64:]
    a1 = along_x(upper, 1)
    a2 = along_x(lower, -1)
    b1 = along_x(lower, 1)
    b2 = along_x(upper, -1)
    f1 = along_x(a1, 1)
    f2 = along_x(a2, -1)
    place = (sp * 512 + jnp.arange(512, dtype=jnp.int32)).astype(F32)
    inverse = 10000.0 ** (-jnp.arange(0, 32, dtype=F32) * 2.0 / 64)
    angles = place[:, None] * inverse[None, :]
    cosine = jnp.cos(angles)
    sine = jnp.sin(angles)
    cos = jnp.concatenate([cosine] * 4, axis=1)
    sin = jnp.concatenate([-sine, sine, -sine, sine], axis=1)
    weights = prefetch(
        (query_weight, key_weight, value_weight, glu_value_weight, glu_gate_weight),
        cos,
        sin,
    )
    shared = (
        norm_gain[None, :],
        *weights,
        qk_gain,
        cos,
        sin,
    )
    mine, gated, given = project(
        project_first, 384, pos, (upper, lower, a1, b1, b2, a2), shared, ()
    )
    near_in = to_mirror(given)
    mine, gated, given = project(project_last, 128, pos, (f1, f2), shared, (mine, gated))
    far_in = to_mirror(given)
    halo = lax.ppermute(
        gated[482:], "sp", [(i, i + 1) for i in range(NZ * NY * NC - 1)]
    )
    q, kv = assemble(pos, mine, near_in, far_in)
    kv1 = send_keys(kv, 1)
    kv2 = send_keys(kv, -1)
    q1 = send_query(q, 1)
    q2 = send_query(q, -1)
    q3 = send_query(q, 2)
    kv3 = send_keys(kv, 2)
    sums = attention_call(own_kernel, (pos, q, kv), (), 1, carried=False, checked=False)
    sums = attention_call(near_kernel, (pos, q, q1, q2, kv, kv1, kv2, *sums), (), 8, checked=False)
    *sums, o1, o2 = attention_call(
        mid_kernel, (pos, q1, q2, kv, kv1, kv2, kv3, *sums), (SENT,) * 2, 2
    )
    r1 = send_query(o1, -1)
    r2 = send_query(o2, 1)
    *sums, o3 = attention_call(far_kernel, (pos, q3, kv, kv1, kv2, kv3, *sums), (SENT,), 4)
    r3 = send_query(o3, 2)
    own, stats = attention_call(
        last_kernel,
        (pos, q, kv, kv1, kv2, kv3, *sums),
        (),
        1,
        carried=False,
        sums=(
            jax.ShapeDtypeStruct((4, 128, 512), F32),
            jax.ShapeDtypeStruct((8, 1024), F32),
        ),
        extra=(pltpu.VMEM((4, 8, 512), F32),),
    )
    conv = convolve(gated, halo, conv_kernel, channel_gain[None, :], channel_shift[None, :])
    conv, stats = lax.optimization_barrier((conv, stats))
    conv = lax.all_to_all(conv, "tp", split_axis=0, concat_axis=0, tiled=True)
    packed, lmine, lother = merge(
        pos,
        mix_lambda,
        own,
        stats,
        (r1, r2, r3),
        head_gain[None, :],
    )
    groups = []
    for z in range(NZ):
        for y in range(NY):
            ends = ((z * NY + y) * NC, ((NZ - 1 - z) * NY + y) * NC + 1)
            groups.append([end * 4 + x for end in ends for x in range(4)])
    moved = lax.all_to_all(
        packed, ("sp", "tp"), split_axis=0, concat_axis=0, axis_index_groups=groups, tiled=True
    )
    ltheirs = to_mirror(lother)
    log_totals = jnp.where(
        core == 0, jnp.stack([lmine, ltheirs], axis=1), jnp.stack([ltheirs, lmine], axis=1)
    )
    part = product(half_kernel, F32, conv, lmine, output_weight)
    mixed = product(output_kernel, BF, moved, part, output_weight)
    return (mixed, log_totals)


def solution(mesh):
    placed = (
        P(("sp", "tp"), None),
        P(),
        P(None, "tp"),
        P(None, "tp"),
        P(None, "tp"),
        P(None, "tp"),
        P(None, "tp"),
        P(),
        P("tp"),
        P(),
        P(None, "tp"),
        P("tp"),
        P("tp"),
        P(),
    )
    return jax.shard_map(
        per_device_steps,
        mesh=mesh,
        in_specs=placed,
        out_specs=(P(("sp", "tp"), None), P(None, "tp", "sp")),
        check_vma=False,
    )
```
